32 devices in a mesh: grp: 2 (over y), kv: 4 (over z), tp: 4 (over x, core).
Axes of the slice: x: 2, y: 2, z: 4, core: 2. Of those that a mesh axis runs over, the one named last changes fastest.
Arguments:
- candidate_embeddings: bfloat16 [1536, 4096], P(('grp', 'kv'), 'tp'), parts along dimension 0, may hold values from -100 to 100
- incoming_rms_scaling: float32 [4096], replicated, may hold values from 0.1 to 1.9
- probe_projector: bfloat16 [4096, 2048], P('kv', 'tp'), may hold values from -0.09375 to 0.09375
- address_projector: bfloat16 [4096, 2048], P('kv', 'tp'), may hold values from -0.09375 to 0.09375
- content_projector: bfloat16 [4096, 2048], P('kv', 'tp'), may hold values from -0.09375 to 0.09375
- sigmoid_mask_matrix: bfloat16 [4096, 2048], P('kv', 'tp'), may hold values from -0.09375 to 0.09375
- forgetting_projector: bfloat16 [4096, 16], replicated, may hold values from -0.09375 to 0.09375
- strength_projector_matrix: bfloat16 [4096, 16], replicated, may hold values from -0.09375 to 0.09375
- channel_forgetting_rates: float32 [16], P('tp'), may hold values from -3 to 0.5
- forgetting_offset: float32 [16], P('tp'), may hold values from -1 to 1
- extra_forgetting: float32 [384, 4, 16], P(('grp', 'kv'), None, 'tp'), parts along dimension 0, may hold values from -0.7 to 0, as said below
- outgoing_rms_scaling: float32 [128], replicated, may hold values from 0.1 to 1.9
- final_projector: bfloat16 [2048, 4096], P('tp', 'kv'), may hold values from -0.125 to 0.125
- memory_matrix: float32 [384, 16, 128, 128], P(('grp', 'kv'), 'tp'), parts along dimension 0, may hold values from -4 to 4
- earlier_addresses: bfloat16 [384, 4, 16, 128], P(('grp', 'kv'), None, 'tp'), parts along dimension 0, may hold values from -6 to 6
- earlier_contents: bfloat16 [384, 4, 16, 128], P(('grp', 'kv'), None, 'tp'), parts along dimension 0, may hold values from -6 to 6
- earlier_strengths: float32 [384, 4, 16], P(('grp', 'kv'), None, 'tp'), parts along dimension 0, may hold values from 0.1 to 0.9
- earlier_forgetting: float32 [384, 4, 16], P(('grp', 'kv'), None, 'tp'), parts along dimension 0, may hold values from -1.5 to -0.02
- admitted_counts: int32 [384], P(('grp', 'kv')), parts along dimension 0, may hold values from 0 to 4
Outputs:
- mixed: bfloat16 [1536, 4096], P(('grp', 'kv'), 'tp'), parts along dimension 0
- taken_state: float32 [384, 16, 128, 128], P(('grp', 'kv'), 'tp'), parts along dimension 0
The draws below stay inside these ranges and needn't reach their ends.
There are 2 independent parts, one for each index of `grp`. The reference program is written for one: setup_inputs(seed, part) draws one part's arguments, and reference() takes and returns one part's arrays. A program takes and returns all parts, laid end to end along the dimension named above; an argument that names none is the same for every part. Nothing has to cross between parts.
Inputs may be any that keep to these rules, and one draw needn't show every extreme that they name: `extra_forgetting`: mostly zero; elsewhere the logarithm of a factor between 0.5 and 0.8.
All inputs are finite; a program needn't handle non-finite values.
Results may differ from the reference program's by a relative error of at most 0.015.
Values may be sent and summed in bfloat16 or wider, within the bound.
A program may use at most 128 MiB of HBM per device.

```python
import math
import jax
import jax.numpy as jnp
from jax import lax

D = 4096
H = 16
DK = 128
P_SIZE = 4
SEQS = 192
ROWS = 768
N_TP = 4


def draw_candidate_embeddings(key, part):
    key = jax.random.fold_in(key, 11)
    key_base, key_rows = jax.random.split(key)
    values_raw = jax.random.truncated_normal(key_base, -4.0, 4.0, (ROWS, D), jnp.float32)
    column = jnp.exp(math.log(10.0) * jnp.arange(D, dtype=jnp.float32) / D)
    row_scale = jnp.exp(jax.random.uniform(key_rows, (ROWS, 1), jnp.float32, 0.0, math.log(10.0)))
    return (values_raw * column[None, :] * row_scale / 4.0).astype(jnp.bfloat16)


def draw_extra_forgetting(key, part):
    key = jax.random.fold_in(key, 23)
    key_where, key_size = jax.random.split(key)
    struck = jax.random.randint(key_where, (SEQS, P_SIZE, H), 0, 8) == 0
    strength = jnp.log(jax.random.uniform(key_size, (SEQS, P_SIZE, H), jnp.float32, 0.5, 0.8))
    return jnp.where(struck, strength, jnp.zeros((SEQS, P_SIZE, H), jnp.float32))


def draw_admitted_counts(key, part):
    key = jax.random.fold_in(key, 37)
    return jax.random.randint(key, (SEQS,), 0, P_SIZE + 1).astype(jnp.int32)


def level_of(own_key, shape, pieces, low, largest):
    level, own = 1.0, jax.random.fold_in(own_key, 6)
    for position, shards_of in pieces:
        draws = jnp.exp(jax.random.uniform(jax.random.fold_in(own, position), (shards_of,), jnp.float32, low / len(pieces), largest / len(pieces)))
        level = level * jnp.repeat(draws, shape[position] // shards_of).reshape([-1 if axis == position else 1 for axis in range(len(shape))])
    return level


def noise(own_key, extent, scale, bound, pieces=(), kind=jnp.bfloat16):
    result = scale * jax.random.normal(own_key, extent, jnp.float32)
    if pieces:
        result = result * level_of(own_key, extent, pieces, -0.22, 0.18)
    return jnp.clip(result, -bound, bound).astype(kind)


def setup_inputs(seed: int = 0, part: int = 0) -> dict:
    seeds = jax.random.split(jax.random.key(seed), 20)
    own_keys = jax.random.split(jax.random.fold_in(seeds[19], part), 20)
    candidate_embeddings = draw_candidate_embeddings(jax.random.fold_in(jax.random.fold_in(seeds[19], part), 71), part)
    incoming_rms_scaling = jnp.clip(1.0 + 0.18 * jax.random.normal(seeds[1], (D,), jnp.float32), 0.1, 1.9)
    probe_projector = noise(seeds[2], (D, H * DK), D ** -0.5, 0.09375, ((0, 4), (1, 4)))
    address_projector = noise(seeds[3], (D, H * DK), D ** -0.5, 0.09375, ((0, 4), (1, 4)))
    content_projector = noise(seeds[4], (D, H * DK), D ** -0.5, 0.09375, ((0, 4), (1, 4)))
    sigmoid_mask_matrix = noise(seeds[5], (D, H * DK), D ** -0.5, 0.09375, ((0, 4), (1, 4)))
    forgetting_projector = noise(seeds[6], (D, H), D ** -0.5, 0.09375)
    strength_projector_matrix = noise(seeds[7], (D, H), D ** -0.5, 0.09375)
    channel_forgetting_rates = jnp.clip(-3.0 + 3.5 * jax.random.uniform(seeds[8], (H,), jnp.float32) ** level_of(seeds[8], (H,), ((0, 4),), -0.2, 0.2), -3.0, 0.5)
    forgetting_offset = jnp.clip(jax.random.uniform(seeds[9], (H,), jnp.float32, -1.0, 1.0) * level_of(seeds[9], (H,), ((0, 4),), -0.4, 0.0), -1.0, 1.0)
    extra_forgetting = draw_extra_forgetting(jax.random.fold_in(jax.random.fold_in(seeds[19], part), 71), part)
    outgoing_rms_scaling = jnp.clip(1.0 + 0.18 * jax.random.normal(seeds[11], (DK,), jnp.float32), 0.1, 1.9)
    final_projector = noise(seeds[12], (H * DK, D), (H * DK) ** -0.5, 0.125, ((0, 4), (1, 4)))
    memory_matrix = noise(own_keys[13], (SEQS, H, DK, DK), 0.25, 4.0, ((0, 4), (1, 4)), jnp.float32)
    earlier_addresses = noise(own_keys[14], (SEQS, P_SIZE, H, DK), 1.0, 6.0, ((0, 4), (2, 4)))
    earlier_contents = noise(own_keys[15], (SEQS, P_SIZE, H, DK), 1.0, 6.0, ((0, 4), (2, 4)))
    earlier_strengths = jnp.clip(0.1 + 0.79999997 * jax.random.uniform(own_keys[16], (SEQS, P_SIZE, H), jnp.float32) ** level_of(own_keys[16], (SEQS, P_SIZE, H), ((0, 4), (2, 4)), -0.2, 0.2), 0.1, 0.9)
    earlier_forgetting = jnp.clip(-1.5 + 1.48 * jax.random.uniform(own_keys[17], (SEQS, P_SIZE, H), jnp.float32) ** level_of(own_keys[17], (SEQS, P_SIZE, H), ((0, 4), (2, 4)), -0.2, 0.2), -1.5, -0.02)
    admitted_counts = draw_admitted_counts(jax.random.fold_in(jax.random.fold_in(seeds[19], part), 71), part)
    return {"candidate_embeddings": candidate_embeddings, "incoming_rms_scaling": incoming_rms_scaling, "probe_projector": probe_projector, "address_projector": address_projector, "content_projector": content_projector, "sigmoid_mask_matrix": sigmoid_mask_matrix, "forgetting_projector": forgetting_projector, "strength_projector_matrix": strength_projector_matrix, "channel_forgetting_rates": channel_forgetting_rates, "forgetting_offset": forgetting_offset, "extra_forgetting": extra_forgetting, "outgoing_rms_scaling": outgoing_rms_scaling, "final_projector": final_projector, "memory_matrix": memory_matrix, "earlier_addresses": earlier_addresses, "earlier_contents": earlier_contents, "earlier_strengths": earlier_strengths, "earlier_forgetting": earlier_forgetting, "admitted_counts": admitted_counts}


epsilon = 1e-06
highest = lax.Precision.HIGHEST

def unit_norm(vector):
    return vector * lax.rsqrt(lax.optimization_barrier(jnp.sum(vector * vector, axis=-1, keepdims=True)) + epsilon)

def update(carry, key_vec, value_vec, beta, log_decay):
    decayed = jnp.exp(log_decay)[..., None, None] * carry
    recalled = jnp.einsum('shde,shd->she', decayed, key_vec, precision=highest)
    return decayed + jnp.einsum('shd,she->shde', key_vec, beta[..., None] * (value_vec - recalled), precision=highest)

def stored(values):
    return lax.optimization_barrier(values.astype(jnp.bfloat16)).astype(jnp.float32)

def reference(candidate_embeddings, incoming_rms_scaling, probe_projector, address_projector, content_projector, sigmoid_mask_matrix, forgetting_projector, strength_projector_matrix, channel_forgetting_rates, forgetting_offset, extra_forgetting, outgoing_rms_scaling, final_projector, memory_matrix, earlier_addresses, earlier_contents, earlier_strengths, earlier_forgetting, admitted_counts):
    floated = candidate_embeddings.astype(jnp.float32)
    normed = (floated * lax.rsqrt(lax.optimization_barrier(jnp.mean(floated * floated, axis=1, keepdims=True)) + epsilon) * incoming_rms_scaling).astype(jnp.bfloat16)

    def project(weight):
        return stored(jnp.dot(normed, weight, preferred_element_type=jnp.float32)).reshape(SEQS, P_SIZE, H, DK)
    query = unit_norm(project(probe_projector)) * DK ** (-0.5)
    keyed = unit_norm(project(address_projector))
    valued = project(content_projector)
    gated = project(sigmoid_mask_matrix)
    forgetting_argument = jnp.dot(normed, forgetting_projector, preferred_element_type=jnp.float32).reshape(SEQS, P_SIZE, H)
    beta_in = jnp.dot(normed, strength_projector_matrix, preferred_element_type=jnp.float32).reshape(SEQS, P_SIZE, H)
    forgetting_multiplier = -jnp.exp(channel_forgetting_rates) * jax.nn.softplus(forgetting_argument + forgetting_offset) + extra_forgetting
    beta = jax.nn.sigmoid(beta_in)
    carried = memory_matrix
    for proposal in range(P_SIZE):
        fresh = update(carried, unit_norm(earlier_addresses[:, proposal].astype(jnp.float32)), earlier_contents[:, proposal].astype(jnp.float32), earlier_strengths[:, proposal], earlier_forgetting[:, proposal])
        live = (admitted_counts > proposal)[:, None, None, None]
        carried = jnp.where(live, fresh, carried)
    running = carried
    outputs = []
    for proposal in range(P_SIZE):
        running = update(running, keyed[:, proposal], valued[:, proposal], beta[:, proposal], forgetting_multiplier[:, proposal])
        outputs.append(jnp.einsum('shde,shd->she', running, query[:, proposal], precision=highest))
    attended = jnp.stack(outputs, axis=1)
    scaled = attended * lax.rsqrt(lax.optimization_barrier(jnp.mean(attended * attended, axis=-1, keepdims=True)) + epsilon) * outgoing_rms_scaling * jax.nn.silu(gated)
    flat = scaled.astype(jnp.bfloat16).reshape(ROWS, N_TP, H * DK // N_TP)
    weights = final_projector.reshape(N_TP, H * DK // N_TP, D)
    partial_value = jnp.einsum('rtc,tcd->rtd', flat.astype(jnp.float32), weights.astype(jnp.float32))
    mixed = lax.optimization_barrier(jnp.sum(stored(partial_value), axis=1)).astype(jnp.bfloat16)
    return (mixed, carried)
```

```python
import functools

import jax
import jax.numpy as jnp
from jax import lax
from jax.experimental import pallas as pl
from jax.experimental.pallas import tpu as pltpu
from jax.sharding import PartitionSpec as P

DK = 128
P_SIZE = 4
SB = 8
TALL = SB * P_SIZE
epsilon = 1e-06
f32 = jnp.float32
bf16 = jnp.bfloat16


def lane_dot(a, b):
    return jnp.sum(a * b, axis=-1, keepdims=True)


def first_half():
    return lax.broadcasted_iota(jnp.int32, (8, DK), 0) < P_SIZE


def load_heads(heads, src, dst):
    for h in range(heads):
        dst[pl.ds(h * TALL, TALL), :] = src[:, h * DK : (h + 1) * DK].astype(f32)


def tile(h, pair):
    return pl.ds(h * TALL + pair * 8, 8)


def proposal(h, p):
    return pl.ds(h * TALL + p, SB, stride=P_SIZE)


def accepted_kernel(heads, s_ref, k_ref, v_ref, f_ref, b_ref, n_ref, o_ref, r_scr, u_scr, c_scr, kf, vf):
    load_heads(heads, k_ref, kf)
    load_heads(heads, v_ref, vf)
    low = first_half()
    for pair in range(SB // 2):
        for h in range(heads):
            at = tile(h, pair)
            lhs = kf[at, :].astype(bf16)
            r0 = jnp.dot(lhs, s_ref[2 * pair, h].astype(bf16), preferred_element_type=f32)
            r1 = jnp.dot(lhs, s_ref[2 * pair + 1, h].astype(bf16), preferred_element_type=f32)
            r_scr[at, :] = jnp.where(low, r0, r1)
    count = n_ref[...]
    for h in range(heads):
        scale = jnp.ones((SB, 1), f32)
        ks, us, norms = [], [], []
        for p in range(P_SIZE):
            at = proposal(h, p)
            col = slice(p * heads + h, p * heads + h + 1)
            key = kf[at, :]
            norm = lax.rsqrt(lane_dot(key, key) + epsilon)
            live = count > p
            g = jnp.where(live, jnp.exp(f_ref[:, col]), 1.0)
            b = jnp.where(live, b_ref[:, col], 0.0)
            rec = (scale * norm) * r_scr[at, :]
            for ki, ui, ni in zip(ks, us, norms):
                rec = rec + (lane_dot(ki, key) * (ni * norm)) * ui
            us = [ui * g for ui in us]
            scale = scale * g
            us.append(b * (vf[at, :] - g * rec))
            ks.append(key)
            norms.append(norm)
        for p in range(P_SIZE):
            u_scr[proposal(h, p), :] = us[p] * norms[p]
        c_scr[pl.ds(h * SB, SB), :] = jnp.broadcast_to(scale, (SB, DK))
    for pair in range(SB // 2):
        for h in range(heads):
            at = tile(h, pair)
            key = kf[at, :]
            lhs = jnp.concatenate([key, key], axis=0).astype(bf16)
            u = u_scr[at, :]
            hi = u.astype(bf16).astype(f32)
            lo = u - hi
            for half in range(2):
                keep = low if half == 0 else jnp.logical_not(low)
                rhs = jnp.concatenate([jnp.where(keep, hi, 0.0), jnp.where(keep, lo, 0.0)], axis=0).astype(bf16)
                seq = 2 * pair + half
                add = lax.dot_general(lhs, rhs, (((0,), (0,)), ((), ())), preferred_element_type=f32)
                o_ref[seq, h] = c_scr[pl.ds(h * SB + seq, 1), :] * s_ref[seq, h] + add


def attend_kernel(heads, s_ref, q_ref, k_ref, v_ref, z_ref, d_ref, b_ref, w_ref, o_ref, rk, rq, qf, kf, vf, zf, of):
    for src, dst in ((q_ref, qf), (k_ref, kf), (v_ref, vf), (z_ref, zf)):
        load_heads(heads, src, dst)
    low = first_half()
    for pair in range(SB // 2):
        for h in range(heads):
            at = tile(h, pair)
            lhs = jnp.concatenate([kf[at, :], qf[at, :]], axis=0).astype(bf16)
            r0 = jnp.dot(lhs, s_ref[2 * pair, h].astype(bf16), preferred_element_type=f32)
            r1 = jnp.dot(lhs, s_ref[2 * pair + 1, h].astype(bf16), preferred_element_type=f32)
            rk[at, :] = jnp.where(low, r0[:8], r1[:8])
            rq[at, :] = jnp.where(low, r0[8:], r1[8:])
    gain = w_ref[...]
    for h in range(heads):
        scale = jnp.ones((SB, 1), f32)
        ks, us, norms = [], [], []
        for p in range(P_SIZE):
            at = proposal(h, p)
            col = slice(p * heads + h, p * heads + h + 1)
            key = kf[at, :]
            query = qf[at, :]
            norm = lax.rsqrt(lane_dot(key, key) + epsilon)
            qnorm = lax.rsqrt(lane_dot(query, query) + epsilon) * DK ** (-0.5)
            g = jnp.exp(d_ref[:, col])
            rec = (scale * norm) * rk[at, :]
            for ki, ui, ni in zip(ks, us, norms):
                rec = rec + (lane_dot(ki, key) * (ni * norm)) * ui
            us = [ui * g for ui in us]
            scale = scale * g
            us.append(b_ref[:, col] * (vf[at, :] - g * rec))
            ks.append(key)
            norms.append(norm)
            att = (scale * qnorm) * rq[at, :]
            for ki, ui, ni in zip(ks, us, norms):
                att = att + (lane_dot(ki, query) * (ni * qnorm)) * ui
            gate = zf[at, :]
            mean = jnp.sum(att * att, axis=-1, keepdims=True) / DK
            of[at, :] = att * lax.rsqrt(mean + epsilon) * gain * (gate * jax.nn.sigmoid(gate))
    for h in range(heads):
        o_ref[:, h * DK : (h + 1) * DK] = of[pl.ds(h * TALL, TALL), :].astype(bf16)


def accepted(state, keys, values, forgetting, strengths, counts):
    seqs, heads = state.shape[:2]
    width = heads * DK
    rows = TALL
    tall = pl.BlockSpec((rows, width), lambda i: (i, 0))
    thin = pl.BlockSpec((SB, P_SIZE * heads), lambda i: (i, 0))
    block = pl.BlockSpec((SB, heads, DK, DK), lambda i: (i, 0, 0, 0))
    return pl.pallas_call(
        functools.partial(accepted_kernel, heads),
        grid=(seqs // SB,),
        in_specs=[block, tall, tall, thin, thin, pl.BlockSpec((SB, 1), lambda i: (i, 0))],
        out_specs=block,
        out_shape=jax.ShapeDtypeStruct(state.shape, f32),
        scratch_shapes=[pltpu.VMEM((heads * n, DK), f32) for n in (TALL, TALL, SB, TALL, TALL)],
        cost_estimate=pl.CostEstimate(flops=10_000_000_000, bytes_accessed=2 * state.size * 4, transcendentals=0),
        name="accepted",
    )(state, keys, values, forgetting, strengths, counts)


def attend(state, packed, decay, beta, gain):
    seqs, heads = state.shape[:2]
    width = heads * DK
    rows = TALL
    thin = pl.BlockSpec((SB, P_SIZE * heads), lambda i: (i, 0))
    block = pl.BlockSpec((SB, heads, DK, DK), lambda i: (i, 0, 0, 0))

    def part(n):
        return pl.BlockSpec((rows, width), lambda i: (i, n))

    return pl.pallas_call(
        functools.partial(attend_kernel, heads),
        grid=(seqs // SB,),
        in_specs=[block, part(0), part(1), part(2), part(3), thin, thin, pl.BlockSpec((1, DK), lambda i: (0, 0))],
        out_specs=pl.BlockSpec((rows, width), lambda i: (i, 0)),
        out_shape=jax.ShapeDtypeStruct((seqs * P_SIZE, width), bf16),
        scratch_shapes=[pltpu.VMEM((heads * TALL, DK), f32)] * 7,
        cost_estimate=pl.CostEstimate(flops=5_000_000_000, bytes_accessed=state.size * 4, transcendentals=0),
        name="attend",
    )(state, packed, packed, packed, packed, decay, beta, gain.reshape(1, DK))


def on_device(
    n_kv,
    n_tp,
    candidate_embeddings,
    incoming_rms_scaling,
    probe_projector,
    address_projector,
    content_projector,
    sigmoid_mask_matrix,
    forgetting_projector,
    strength_projector_matrix,
    channel_forgetting_rates,
    forgetting_offset,
    extra_forgetting,
    outgoing_rms_scaling,
    final_projector,
    memory_matrix,
    earlier_addresses,
    earlier_contents,
    earlier_strengths,
    earlier_forgetting,
    admitted_counts,
):
    rows, local_cols = candidate_embeddings.shape
    features = incoming_rms_scaling.shape[0]
    depth, width = probe_projector.shape
    heads = width // DK
    seqs = rows // P_SIZE
    square = n_kv == n_tp
    swap = [(a * n_tp + b, b * n_tp + a) for a in range(n_kv) for b in range(n_tp)] if square else None
    k_index, t_index = lax.axis_index("kv"), lax.axis_index("tp")

    def thin(values):
        return values.reshape(seqs, P_SIZE * heads)

    if square:
        turned = lax.ppermute(candidate_embeddings, ("kv", "tp"), swap)
        every = lax.all_gather(turned, "tp", axis=0, tiled=True)
    else:
        every = lax.all_gather(candidate_embeddings, "tp", axis=1, tiled=True)
        every = lax.all_to_all(every, "kv", split_axis=1, concat_axis=0, tiled=True)
    gain_part = lax.dynamic_slice_in_dim(incoming_rms_scaling, k_index * depth, depth)
    floated = every.astype(f32)
    gained = (floated * gain_part).astype(bf16)
    decay_cols = lax.dynamic_slice(forgetting_projector, (k_index * depth, t_index * heads), (depth, heads))
    beta_cols = lax.dynamic_slice(strength_projector_matrix, (k_index * depth, t_index * heads), (depth, heads))
    few = jnp.concatenate(
        [
            jnp.dot(gained, jnp.concatenate([decay_cols, beta_cols], axis=1), preferred_element_type=f32),
            jnp.sum(floated * floated, axis=1, keepdims=True),
        ],
        axis=1,
    )
    few = lax.psum_scatter(few, "kv", scatter_dimension=0, tiled=True)
    partial = jnp.concatenate(
        [
            jnp.dot(gained, w, preferred_element_type=f32).astype(bf16)
            for w in (probe_projector, address_projector, content_projector, sigmoid_mask_matrix)
        ],
        axis=1,
    )
    summed = lax.psum_scatter(partial, "kv", scatter_dimension=0, tiled=True)
    taken = accepted(
        memory_matrix,
        earlier_addresses.reshape(rows, width),
        earlier_contents.reshape(rows, width),
        thin(earlier_forgetting),
        thin(earlier_strengths),
        admitted_counts.reshape(seqs, 1),
    )
    factor = lax.rsqrt(few[:, 2 * heads :] / features + epsilon)
    few = few[:, : 2 * heads] * factor
    packed = (summed.astype(f32) * factor).astype(bf16)
    decay_in = few[:, :heads].reshape(seqs, P_SIZE, heads)
    beta = jax.nn.sigmoid(few[:, heads:].reshape(seqs, P_SIZE, heads))
    decay = -jnp.exp(channel_forgetting_rates) * jax.nn.softplus(decay_in + forgetting_offset) + extra_forgetting
    flat = attend(taken, packed, thin(decay), thin(beta), outgoing_rms_scaling)
    gathered = lax.all_gather(flat, "kv", axis=0, tiled=True)
    terms = jnp.dot(gathered, final_projector, preferred_element_type=f32).astype(bf16)
    if square:
        mixed = lax.psum_scatter(terms, "tp", scatter_dimension=0, tiled=True)
        mixed = lax.ppermute(mixed, ("kv", "tp"), swap)
    else:
        terms = lax.all_to_all(terms, "kv", split_axis=0, concat_axis=1, tiled=True)
        mixed = lax.psum_scatter(terms, "tp", scatter_dimension=1, tiled=True)
    return (mixed, taken)


def solution(mesh):
    row, per_head = P(("grp", "kv"), "tp"), P(("grp", "kv"), None, "tp")
    four = P(("grp", "kv"), None, "tp", None)
    weight = P("kv", "tp")
    state = P(("grp", "kv"), "tp", None, None)
    in_specs = (
        row, P(), weight, weight, weight, weight, P(), P(), P("tp"), P("tp"), per_head, P(),
        P("tp", "kv"), state, four, four, per_head, per_head, P(("grp", "kv")),
    )
    body = functools.partial(on_device, mesh.shape["kv"], mesh.shape["tp"])
    return jax.shard_map(body, mesh=mesh, in_specs=in_specs, out_specs=(row, state), check_vma=False)
```

```python
import functools

import jax
import jax.numpy as jnp
from jax import lax
from jax.experimental import pallas as pl
from jax.experimental.pallas import tpu as pltpu
from jax.sharding import PartitionSpec as P

DK = 128
P_SIZE = 4
SB = 8
TALL = SB * P_SIZE
epsilon = 1e-06
f32 = jnp.float32
bf16 = jnp.bfloat16


def lane_dot(a, b):
    return jnp.sum(a * b, axis=-1, keepdims=True)


def first_half():
    return lax.broadcasted_iota(jnp.int32, (8, DK), 0) < P_SIZE


def load_heads(heads, src, dst, factor=None):
    for h in range(heads):
        part = src[:, h * DK : (h + 1) * DK].astype(f32)
        dst[pl.ds(h * TALL, TALL), :] = part if factor is None else (part * factor).astype(bf16).astype(f32)


def tile(h, pair):
    return pl.ds(h * TALL + pair * 8, 8)


def proposal(h, p):
    return pl.ds(h * TALL + p, SB, stride=P_SIZE)


def accepted_kernel(heads, s_ref, k_ref, v_ref, f_ref, b_ref, n_ref, o_ref, r_scr, u_scr, c_scr, kf, vf):
    load_heads(heads, k_ref, kf)
    load_heads(heads, v_ref, vf)
    low = first_half()
    for pair in range(SB // 2):
        for h in range(heads):
            at = tile(h, pair)
            lhs = kf[at, :].astype(bf16)
            r0 = jnp.dot(lhs, s_ref[2 * pair, h].astype(bf16), preferred_element_type=f32)
            r1 = jnp.dot(lhs, s_ref[2 * pair + 1, h].astype(bf16), preferred_element_type=f32)
            r_scr[at, :] = jnp.where(low, r0, r1)
    count = n_ref[...]
    for h in range(heads):
        scale = jnp.ones((SB, 1), f32)
        ks, us, norms = [], [], []
        for p in range(P_SIZE):
            at = proposal(h, p)
            col = slice(p * heads + h, p * heads + h + 1)
            key = kf[at, :]
            norm = lax.rsqrt(lane_dot(key, key) + epsilon)
            live = count > p
            g = jnp.where(live, jnp.exp(f_ref[:, col]), 1.0)
            b = jnp.where(live, b_ref[:, col], 0.0)
            rec = (scale * norm) * r_scr[at, :]
            for ki, ui, ni in zip(ks, us, norms):
                rec = rec + (lane_dot(ki, key) * (ni * norm)) * ui
            us = [ui * g for ui in us]
            scale = scale * g
            us.append(b * (vf[at, :] - g * rec))
            ks.append(key)
            norms.append(norm)
        for p in range(P_SIZE):
            u_scr[proposal(h, p), :] = us[p] * norms[p]
        c_scr[pl.ds(h * SB, SB), :] = jnp.broadcast_to(scale, (SB, DK))
    for pair in range(SB // 2):
        for h in range(heads):
            at = tile(h, pair)
            key = kf[at, :]
            lhs = jnp.concatenate([key, key], axis=0).astype(bf16)
            u = u_scr[at, :]
            hi = u.astype(bf16).astype(f32)
            lo = u - hi
            for half in range(2):
                keep = low if half == 0 else jnp.logical_not(low)
                rhs = jnp.concatenate([jnp.where(keep, hi, 0.0), jnp.where(keep, lo, 0.0)], axis=0).astype(bf16)
                seq = 2 * pair + half
                add = lax.dot_general(lhs, rhs, (((0,), (0,)), ((), ())), preferred_element_type=f32)
                o_ref[seq, h] = c_scr[pl.ds(h * SB + seq, 1), :] * s_ref[seq, h] + add


def attend_kernel(heads, s_ref, a_ref, q_ref, k_ref, v_ref, z_ref, d_ref, b_ref, w_ref, o_ref, rk, rq, qf, kf, vf, zf, of):
    for src, dst in ((q_ref, qf), (k_ref, kf), (v_ref, vf), (z_ref, zf)):
        load_heads(heads, src, dst, a_ref[...])
    low = first_half()
    for pair in range(SB // 2):
        for h in range(heads):
            at = tile(h, pair)
            lhs = jnp.concatenate([kf[at, :], qf[at, :]], axis=0).astype(bf16)
            r0 = jnp.dot(lhs, s_ref[2 * pair, h].astype(bf16), preferred_element_type=f32)
            r1 = jnp.dot(lhs, s_ref[2 * pair + 1, h].astype(bf16), preferred_element_type=f32)
            rk[at, :] = jnp.where(low, r0[:8], r1[:8])
            rq[at, :] = jnp.where(low, r0[8:], r1[8:])
    gain = w_ref[...]
    for h in range(heads):
        scale = jnp.ones((SB, 1), f32)
        ks, us, norms = [], [], []
        for p in range(P_SIZE):
            at = proposal(h, p)
            col = slice(p * heads + h, p * heads + h + 1)
            key = kf[at, :]
            query = qf[at, :]
            norm = lax.rsqrt(lane_dot(key, key) + epsilon)
            qnorm = lax.rsqrt(lane_dot(query, query) + epsilon) * DK ** (-0.5)
            g = jnp.exp(d_ref[:, col])
            rec = (scale * norm) * rk[at, :]
            for ki, ui, ni in zip(ks, us, norms):
                rec = rec + (lane_dot(ki, key) * (ni * norm)) * ui
            us = [ui * g for ui in us]
            scale = scale * g
            us.append(b_ref[:, col] * (vf[at, :] - g * rec))
            ks.append(key)
            norms.append(norm)
            att = (scale * qnorm) * rq[at, :]
            for ki, ui, ni in zip(ks, us, norms):
                att = att + (lane_dot(ki, query) * (ni * qnorm)) * ui
            gate = zf[at, :]
            mean = jnp.sum(att * att, axis=-1, keepdims=True) / DK
            of[at, :] = att * lax.rsqrt(mean + epsilon) * gain * (gate * jax.nn.sigmoid(gate))
    for h in range(heads):
        o_ref[:, h * DK : (h + 1) * DK] = of[pl.ds(h * TALL, TALL), :].astype(bf16)


def accepted(state, keys, values, forgetting, strengths, counts):
    seqs, heads = state.shape[:2]
    width = heads * DK
    rows = TALL
    tall = pl.BlockSpec((rows, width), lambda i: (i, 0))
    thin = pl.BlockSpec((SB, P_SIZE * heads), lambda i: (i, 0))
    block = pl.BlockSpec((SB, heads, DK, DK), lambda i: (i, 0, 0, 0))
    return pl.pallas_call(
        functools.partial(accepted_kernel, heads),
        grid=(seqs // SB,),
        in_specs=[block, tall, tall, thin, thin, pl.BlockSpec((SB, 1), lambda i: (i, 0))],
        out_specs=block,
        out_shape=jax.ShapeDtypeStruct(state.shape, f32),
        scratch_shapes=[pltpu.VMEM((heads * n, DK), f32) for n in (TALL, TALL, SB, TALL, TALL)],
        cost_estimate=pl.CostEstimate(flops=10_000_000_000, bytes_accessed=2 * state.size * 4, transcendentals=0),
        name="accepted",
    )(state, keys, values, forgetting, strengths, counts)


def attend(state, packed, factor, decay, beta, gain):
    seqs, heads = state.shape[:2]
    width = heads * DK
    rows = TALL
    thin = pl.BlockSpec((SB, P_SIZE * heads), lambda i: (i, 0))
    block = pl.BlockSpec((SB, heads, DK, DK), lambda i: (i, 0, 0, 0))

    def part(n):
        return pl.BlockSpec((rows, width), lambda i: (i, n))

    return pl.pallas_call(
        functools.partial(attend_kernel, heads),
        grid=(seqs // SB,),
        in_specs=[block, pl.BlockSpec((rows, 1), lambda i: (i, 0)), part(0), part(1), part(2), part(3), thin, thin, pl.BlockSpec((1, DK), lambda i: (0, 0))],
        out_specs=pl.BlockSpec((rows, width), lambda i: (i, 0)),
        out_shape=jax.ShapeDtypeStruct((seqs * P_SIZE, width), bf16),
        scratch_shapes=[pltpu.VMEM((heads * TALL, DK), f32)] * 7,
        cost_estimate=pl.CostEstimate(flops=5_000_000_000, bytes_accessed=state.size * 4, transcendentals=0),
        name="attend",
    )(state, factor, packed, packed, packed, packed, decay, beta, gain.reshape(1, DK))


def pick(index, values):
    chosen = values[-1]
    for at, value in enumerate(values[:-1]):
        chosen = jnp.where(index == at, value, chosen)
    return chosen


def turned_slot(t):
    return pick(t, (0, 2, 1, 3))


ORDER = ((3, 2, 1, 0), (0, 2, 1, 3), (3, 1, 2, 0), (0, 1, 2, 3))


def project_kernel(x_ref, gain_ref, wq, wk, wv, wz, wf, ws, acc, few_ref, xbuf, w, fs, send, recv, esend, erecv,
                   xs, xr, wsem, ps, pr, es, er):
    k, t, g = lax.axis_index("kv"), lax.axis_index("tp"), lax.axis_index("grp")
    depth, width = w.shape[1], w.shape[2]
    rows = x_ref.shape[0]

    def at(kv, tp):
        return {"grp": g, "kv": kv, "tp": tp}

    def remote(src, dst, ss, rs, kv, tp):
        return pltpu.make_async_remote_copy(src, dst, ss, rs, device_id=at(kv, tp), device_id_type=pl.DeviceIdType.MESH)

    loads = [pltpu.make_async_copy(src, w.at[i], wsem.at[i]) for i, src in enumerate((wq, wk, wv, wz))]
    here = pl.ds(k * depth, depth)
    loads += [pltpu.make_async_copy(src.at[here], fs.at[i], wsem.at[4 + i]) for i, src in enumerate((wf, ws))]
    slot = turned_slot(t)
    far_t, far_k = turned_slot(k), t
    home = jnp.logical_and(far_k == k, far_t == t)
    first = remote(x_ref, xbuf.at[k], xs.at[0], xr.at[k], far_k, far_t)
    local = pltpu.make_async_copy(x_ref, xbuf.at[k], xr.at[k])

    @pl.when(jnp.logical_not(home))
    def _():
        first.start()

    @pl.when(home)
    def _():
        local.start()

    for load in loads:
        load.start()

    beside = t + 1 - 2 * (t % 2)
    across = (t + 2) % 4

    def arrived(s):
        remote(xbuf.at[s], xbuf.at[s], xs.at[0], xr.at[s], k, beside).wait_recv()

    @pl.when(home)
    def _():
        local.wait()

    @pl.when(jnp.logical_not(home))
    def _():
        arrived(slot)

    over = remote(xbuf.at[slot], xbuf.at[slot], xs.at[1], xr.at[slot], k, across)
    over.start()
    near = remote(xbuf.at[slot], xbuf.at[slot], xs.at[2], xr.at[slot], k, beside)
    near.start()
    other = turned_slot(across)
    arrived(other)
    onward = remote(xbuf.at[other], xbuf.at[other], xs.at[3], xr.at[other], k, beside)
    onward.start()
    arrived(turned_slot(beside))
    arrived(turned_slot((beside + 2) % 4))
    for load in loads:
        load.wait()

    def step(i, carry):
        r = pick(k, [pick(i, row) for row in ORDER])
        own = r == k
        floated = xbuf[r].astype(f32)
        gained = (floated * gain_ref[k]).astype(bf16)
        squares = floated * floated
        high = squares.astype(bf16)
        rest = (squares - high.astype(f32)).astype(bf16)
        ones = jnp.ones((8, depth), bf16)
        nt = (((1,), (1,)), ((), ()))
        tn = (((0,), (1,)), ((), ()))
        esend[r, 0:16, :] = lax.dot_general(fs[0], gained, tn, preferred_element_type=f32)
        esend[r, 16:32, :] = lax.dot_general(fs[1], gained, tn, preferred_element_type=f32)
        esend[r, 32:40, :] = lax.dot_general(ones, high, nt, preferred_element_type=f32) + lax.dot_general(
            ones, rest, nt, preferred_element_type=f32
        )
        for j in range(4):
            part = jnp.dot(gained, w[j], preferred_element_type=f32)
            cols = slice(j * width, (j + 1) * width)

            @pl.when(own)
            def _():
                acc[:, cols] = part

            @pl.when(jnp.logical_not(own))
            def _():
                send[r, :, cols] = part.astype(bf16)

        relayed = jnp.logical_or(jnp.logical_and(k == 1, r == 3), jnp.logical_and(k == 2, r == 0))

        @pl.when(relayed)
        def _():
            remote(send.at[r], recv.at[4], ps.at[r], pr.at[4], k, beside).wait_recv()

            def add(c, carry):
                at_rows = pl.ds(c * 16, 16)
                send[r, at_rows, :] = (send[r, at_rows, :].astype(f32) + recv[4, at_rows, :].astype(f32)).astype(bf16)
                return carry

            lax.fori_loop(0, rows // 16, add, 0)

        @pl.when(jnp.logical_not(own))
        def _():
            ends = jnp.logical_or(jnp.logical_and(k == 0, r == 3), jnp.logical_and(k == 3, r == 0))
            target = jnp.where(ends, jnp.where(k == 0, 1, 2), r)
            place = jnp.where(ends, 4, k)
            remote(send.at[r], recv.at[place], ps.at[r], pr.at[place], target, t).start()
            remote(esend.at[r], erecv.at[k], es.at[r], er.at[k], r, t).start()

        return carry

    lax.fori_loop(0, 4, step, 0)

    first_wait = jnp.logical_not(home)

    @pl.when(first_wait)
    def _():
        first.wait_send()

    over.wait_send()
    near.wait_send()
    onward.wait_send()

    few_ref[...] = esend[k]
    for src in range(4):

        @pl.when(k != src)
        def _():
            remote(esend.at[src], erecv.at[src], es.at[src], er.at[src], k, beside).wait()
            few_ref[...] += erecv[src]
            remote(send.at[src], recv.at[src], ps.at[src], pr.at[src], k, beside).wait_send()

        @pl.when(jnp.logical_and(k != src, k + src != 3) if src in (0, 3) else k != src)
        def _():
            remote(send.at[src], recv.at[src], ps.at[src], pr.at[src], k, beside).wait_recv()

            def add(c, carry):
                at_rows = pl.ds(c * 16, 16)
                acc[at_rows, :] = acc[at_rows, :] + recv[src, at_rows, :].astype(f32)
                return carry

            lax.fori_loop(0, rows // 16, add, 0)


def project(x, gain, weights, forgetting, strength):
    rows, depth = x.shape
    width = weights[0].shape[1]
    vmem, hbm = pl.BlockSpec(memory_space=pltpu.VMEM), pl.BlockSpec(memory_space=pl.ANY)
    dma = pltpu.SemaphoreType.DMA
    return pl.pallas_call(
        project_kernel,
        in_specs=[vmem, vmem] + [hbm] * 6,
        out_specs=[vmem, vmem],
        out_shape=[jax.ShapeDtypeStruct((rows, 4 * width), f32), jax.ShapeDtypeStruct((40, rows), f32)],
        scratch_shapes=[
            pltpu.VMEM((4, rows, depth), bf16),
            pltpu.VMEM((4, depth, width), bf16),
            pltpu.VMEM((2,) + (depth, forgetting.shape[1]), bf16),
            pltpu.VMEM((4, rows, 4 * width), bf16),
            pltpu.VMEM((5, rows, 4 * width), bf16),
            pltpu.VMEM((4, 40, rows), f32),
            pltpu.VMEM((4, 40, rows), f32),
            dma((4,)), dma((4,)), dma((6,)), dma((4,)), dma((5,)), dma((4,)), dma((4,)),
        ],
        compiler_params=pltpu.CompilerParams(has_side_effects=True, vmem_limit_bytes=56 * 2**20),
        name="project",
    )(x, gain.reshape(-1, 1, depth), *weights, forgetting, strength)


def on_device(
    n_kv,
    n_tp,
    candidate_embeddings,
    incoming_rms_scaling,
    probe_projector,
    address_projector,
    content_projector,
    sigmoid_mask_matrix,
    forgetting_projector,
    strength_projector_matrix,
    channel_forgetting_rates,
    forgetting_offset,
    extra_forgetting,
    outgoing_rms_scaling,
    final_projector,
    memory_matrix,
    earlier_addresses,
    earlier_contents,
    earlier_strengths,
    earlier_forgetting,
    admitted_counts,
):
    rows, local_cols = candidate_embeddings.shape
    features = incoming_rms_scaling.shape[0]
    depth, width = probe_projector.shape
    heads = width // DK
    seqs = rows // P_SIZE
    square = n_kv == n_tp
    swap = [(a * n_tp + b, b * n_tp + a) for a in range(n_kv) for b in range(n_tp)] if square else None
    k_index, t_index = lax.axis_index("kv"), lax.axis_index("tp")

    def thin(values):
        return values.reshape(seqs, P_SIZE * heads)

    weights = (probe_projector, address_projector, content_projector, sigmoid_mask_matrix)
    if n_kv == 4 and n_tp == 4:
        summed, few = project(
            candidate_embeddings, incoming_rms_scaling, weights, forgetting_projector, strength_projector_matrix
        )
        columns = forgetting_projector.shape[1]
        few = [lax.dynamic_slice_in_dim(few, n * columns + t_index * heads, heads) for n in range(2)] + [few[2 * columns : 2 * columns + 1]]
        few = jnp.concatenate(few, axis=0).T
    else:
        every = lax.all_gather(candidate_embeddings, "tp", axis=1, tiled=True)
        every = lax.all_to_all(every, "kv", split_axis=1, concat_axis=0, tiled=True)
        gain_part = lax.dynamic_slice_in_dim(incoming_rms_scaling, k_index * depth, depth)
        floated = every.astype(f32)
        gained = (floated * gain_part).astype(bf16)
        decay_cols = lax.dynamic_slice(forgetting_projector, (k_index * depth, t_index * heads), (depth, heads))
        beta_cols = lax.dynamic_slice(strength_projector_matrix, (k_index * depth, t_index * heads), (depth, heads))
        few = jnp.concatenate(
            [
                jnp.dot(gained, jnp.concatenate([decay_cols, beta_cols], axis=1), preferred_element_type=f32),
                jnp.sum(floated * floated, axis=1, keepdims=True),
            ],
            axis=1,
        )
        few = lax.psum_scatter(few, "kv", scatter_dimension=0, tiled=True)
        partial = jnp.concatenate(
            [jnp.dot(gained, w, preferred_element_type=f32).astype(bf16) for w in weights], axis=1
        )
        summed = lax.psum_scatter(partial, "kv", scatter_dimension=0, tiled=True).astype(f32)
    taken = accepted(
        memory_matrix,
        earlier_addresses.reshape(rows, width),
        earlier_contents.reshape(rows, width),
        thin(earlier_forgetting),
        thin(earlier_strengths),
        admitted_counts.reshape(seqs, 1),
    )
    factor = lax.rsqrt(few[:, 2 * heads :] / features + epsilon)
    few = few[:, : 2 * heads] * factor
    decay_in = few[:, :heads].reshape(seqs, P_SIZE, heads)
    beta = jax.nn.sigmoid(few[:, heads:].reshape(seqs, P_SIZE, heads))
    decay = -jnp.exp(channel_forgetting_rates) * jax.nn.softplus(decay_in + forgetting_offset) + extra_forgetting
    flat = attend(taken, summed, factor, thin(decay), thin(beta), outgoing_rms_scaling)
    gathered = lax.all_gather(flat, "kv", axis=0, tiled=True)
    terms = jnp.dot(gathered, final_projector, preferred_element_type=f32).astype(bf16)
    if square:
        mixed = lax.psum_scatter(terms, "tp", scatter_dimension=0, tiled=True)
        mixed = lax.ppermute(mixed, ("kv", "tp"), swap)
    else:
        terms = lax.all_to_all(terms, "kv", split_axis=0, concat_axis=1, tiled=True)
        mixed = lax.psum_scatter(terms, "tp", scatter_dimension=1, tiled=True)
    return (mixed, taken)


def solution(mesh):
    row, per_head = P(("grp", "kv"), "tp"), P(("grp", "kv"), None, "tp")
    four = P(("grp", "kv"), None, "tp", None)
    weight = P("kv", "tp")
    state = P(("grp", "kv"), "tp", None, None)
    in_specs = (
        row, P(), weight, weight, weight, weight, P(), P(), P("tp"), P("tp"), per_head, P(),
        P("tp", "kv"), state, four, four, per_head, per_head, P(("grp", "kv")),
    )
    body = functools.partial(on_device, mesh.shape["kv"], mesh.shape["tp"])
    return jax.shard_map(body, mesh=mesh, in_specs=in_specs, out_specs=(row, state), check_vma=False)
```

```python
import functools

import jax
import jax.numpy as jnp
from jax import lax
from jax.experimental import pallas as pl
from jax.experimental.pallas import tpu as pltpu
from jax.sharding import PartitionSpec as P

DK = 128
P_SIZE = 4
SB = 8
TALL = SB * P_SIZE
epsilon = 1e-06
f32 = jnp.float32
bf16 = jnp.bfloat16


def lane_dot(a, b):
    return jnp.sum(a * b, axis=-1, keepdims=True)


def first_half():
    return lax.broadcasted_iota(jnp.int32, (8, DK), 0) < P_SIZE


def load_heads(heads, src, dst, factor=None):
    for h in range(heads):
        part = src[:, h * DK : (h + 1) * DK].astype(f32)
        dst[pl.ds(h * TALL, TALL), :] = part if factor is None else (part * factor).astype(bf16).astype(f32)


def tile(h, pair):
    return pl.ds(h * TALL + pair * 8, 8)


def proposal(h, p):
    return pl.ds(h * TALL + p, SB, stride=P_SIZE)


def accepted_kernel(heads, s_ref, k_ref, v_ref, n_ref, o_ref, r_scr, u_scr, c_scr, kf, vf):
    load_heads(heads, k_ref, kf)
    load_heads(heads, v_ref, vf)
    low = first_half()
    for pair in range(SB // 2):
        for h in range(heads):
            at = tile(h, pair)
            lhs = kf[at, :].astype(bf16)
            r0 = jnp.dot(lhs, s_ref[2 * pair, h].astype(bf16), preferred_element_type=f32)
            r1 = jnp.dot(lhs, s_ref[2 * pair + 1, h].astype(bf16), preferred_element_type=f32)
            r_scr[at, :] = jnp.where(low, r0, r1)
    few = n_ref[...]
    span = P_SIZE * heads
    count = few[:, 2 * span : 2 * span + 1]
    for h in range(heads):
        scale = jnp.ones((SB, 1), f32)
        ks, us, norms = [], [], []
        for p in range(P_SIZE):
            at = proposal(h, p)
            col = slice(p * heads + h, p * heads + h + 1)
            key = kf[at, :]
            norm = lax.rsqrt(lane_dot(key, key) + epsilon)
            live = count > float(p)
            g = jnp.where(live, jnp.exp(few[:, p * heads + h : p * heads + h + 1]), 1.0)
            b = jnp.where(live, few[:, span + p * heads + h : span + p * heads + h + 1], 0.0)
            rec = (scale * norm) * r_scr[at, :]
            for ki, ui, ni in zip(ks, us, norms):
                rec = rec + (lane_dot(ki, key) * (ni * norm)) * ui
            us = [ui * g for ui in us]
            scale = scale * g
            us.append(b * (vf[at, :] - g * rec))
            ks.append(key)
            norms.append(norm)
        for p in range(P_SIZE):
            u_scr[proposal(h, p), :] = us[p] * norms[p]
        c_scr[pl.ds(h * SB, SB), :] = jnp.broadcast_to(scale, (SB, DK))
    for pair in range(SB // 2):
        for h in range(heads):
            at = tile(h, pair)
            key = kf[at, :]
            lhs = jnp.concatenate([key, key], axis=0).astype(bf16)
            u = u_scr[at, :]
            hi = u.astype(bf16).astype(f32)
            lo = u - hi
            for half in range(2):
                keep = low if half == 0 else jnp.logical_not(low)
                rhs = jnp.concatenate([jnp.where(keep, hi, 0.0), jnp.where(keep, lo, 0.0)], axis=0).astype(bf16)
                seq = 2 * pair + half
                add = lax.dot_general(lhs, rhs, (((0,), (0,)), ((), ())), preferred_element_type=f32)
                o_ref[seq, h] = c_scr[pl.ds(h * SB + seq, 1), :] * s_ref[seq, h] + add


def attend_kernel(heads, s_ref, a_ref, q_ref, k_ref, v_ref, z_ref, d_ref, b_ref, w_ref, o_ref, rk, rq, qf, kf, vf, zf, of):
    for src, dst in ((q_ref, qf), (k_ref, kf), (v_ref, vf), (z_ref, zf)):
        load_heads(heads, src, dst, a_ref[...])
    low = first_half()
    for pair in range(SB // 2):
        for h in range(heads):
            at = tile(h, pair)
            lhs = jnp.concatenate([kf[at, :], qf[at, :]], axis=0).astype(bf16)
            r0 = jnp.dot(lhs, s_ref[2 * pair, h].astype(bf16), preferred_element_type=f32)
            r1 = jnp.dot(lhs, s_ref[2 * pair + 1, h].astype(bf16), preferred_element_type=f32)
            rk[at, :] = jnp.where(low, r0[:8], r1[:8])
            rq[at, :] = jnp.where(low, r0[8:], r1[8:])
    gain = w_ref[...]
    for h in range(heads):
        scale = jnp.ones((SB, 1), f32)
        ks, us, norms = [], [], []
        for p in range(P_SIZE):
            at = proposal(h, p)
            col = slice(p * heads + h, p * heads + h + 1)
            key = kf[at, :]
            query = qf[at, :]
            norm = lax.rsqrt(lane_dot(key, key) + epsilon)
            qnorm = lax.rsqrt(lane_dot(query, query) + epsilon) * DK ** (-0.5)
            g = jnp.exp(d_ref[:, col])
            rec = (scale * norm) * rk[at, :]
            for ki, ui, ni in zip(ks, us, norms):
                rec = rec + (lane_dot(ki, key) * (ni * norm)) * ui
            us = [ui * g for ui in us]
            scale = scale * g
            us.append(b_ref[:, col] * (vf[at, :] - g * rec))
            ks.append(key)
            norms.append(norm)
            att = (scale * qnorm) * rq[at, :]
            for ki, ui, ni in zip(ks, us, norms):
                att = att + (lane_dot(ki, query) * (ni * qnorm)) * ui
            gate = zf[at, :]
            mean = jnp.sum(att * att, axis=-1, keepdims=True) / DK
            of[at, :] = att * lax.rsqrt(mean + epsilon) * gain * (gate * jax.nn.sigmoid(gate))
    for h in range(heads):
        o_ref[:, h * DK : (h + 1) * DK] = of[pl.ds(h * TALL, TALL), :].astype(bf16)


def accepted(state, keys, values, few):
    seqs, heads = state.shape[:2]
    width = heads * DK
    rows = TALL
    tall = pl.BlockSpec((rows, width), lambda i: (i, 0))
    thin = pl.BlockSpec((SB, few.shape[1]), lambda i: (i, 0))
    block = pl.BlockSpec((SB, heads, DK, DK), lambda i: (i, 0, 0, 0))
    return pl.pallas_call(
        functools.partial(accepted_kernel, heads),
        grid=(seqs // SB,),
        in_specs=[block, tall, tall, thin],
        out_specs=block,
        out_shape=jax.ShapeDtypeStruct(state.shape, f32),
        scratch_shapes=[pltpu.VMEM((heads * n, DK), f32) for n in (TALL, TALL, SB, TALL, TALL)],
        cost_estimate=pl.CostEstimate(flops=10_000_000_000, bytes_accessed=2 * state.size * 4, transcendentals=0),
        name="accepted",
    )(state, keys, values, few)


def attend(state, packed, factor, decay, beta, gain):
    seqs, heads = state.shape[:2]
    width = heads * DK
    rows = TALL
    thin = pl.BlockSpec((SB, P_SIZE * heads), lambda i: (i, 0))
    block = pl.BlockSpec((SB, heads, DK, DK), lambda i: (i, 0, 0, 0))

    def part(n):
        return pl.BlockSpec((rows, width), lambda i: (i, n))

    return pl.pallas_call(
        functools.partial(attend_kernel, heads),
        grid=(seqs // SB,),
        in_specs=[block, pl.BlockSpec((rows, 1), lambda i: (i, 0)), part(0), part(1), part(2), part(3), thin, thin, pl.BlockSpec((1, DK), lambda i: (0, 0))],
        out_specs=pl.BlockSpec((rows, width), lambda i: (i, 0)),
        out_shape=jax.ShapeDtypeStruct((seqs * P_SIZE, width), bf16),
        scratch_shapes=[pltpu.VMEM((heads * TALL, DK), f32)] * 7,
        cost_estimate=pl.CostEstimate(flops=5_000_000_000, bytes_accessed=state.size * 4, transcendentals=0),
        name="attend",
    )(state, factor, packed, packed, packed, packed, decay, beta, gain.reshape(1, DK))


def pick(index, values):
    chosen = values[-1]
    for at, value in enumerate(values[:-1]):
        chosen = jnp.where(index == at, value, chosen)
    return chosen


def turned_slot(t):
    return pick(t, (0, 2, 1, 3))


ORDER = ((3, 2, 1, 0), (0, 2, 1, 3), (3, 1, 2, 0), (0, 1, 2, 3))


def project_kernel(x_ref, gain_ref, wq, wk, wv, wz, wf, ws, acc, few_ref, xbuf, w, fs, send, recv, esend, erecv,
                   xs, xr, wsem, ps, pr, es, er):
    k, t, g = lax.axis_index("kv"), lax.axis_index("tp"), lax.axis_index("grp")
    depth, width = w.shape[1], w.shape[2]
    rows = x_ref.shape[0]

    def at(kv, tp):
        return {"grp": g, "kv": kv, "tp": tp}

    def remote(src, dst, ss, rs, kv, tp):
        return pltpu.make_async_remote_copy(src, dst, ss, rs, device_id=at(kv, tp), device_id_type=pl.DeviceIdType.MESH)

    loads = [pltpu.make_async_copy(src, w.at[i], wsem.at[i]) for i, src in enumerate((wq, wk, wv, wz))]
    here = pl.ds(k * depth, depth)
    loads += [pltpu.make_async_copy(src.at[:, here], fs.at[i], wsem.at[4 + i]) for i, src in enumerate((wf, ws))]
    slot = turned_slot(t)
    far_t, far_k = turned_slot(k), t
    home = jnp.logical_and(far_k == k, far_t == t)
    first = remote(x_ref, xbuf.at[k], xs.at[0], xr.at[k], far_k, far_t)
    local = pltpu.make_async_copy(x_ref, xbuf.at[k], xr.at[k])

    @pl.when(jnp.logical_not(home))
    def _():
        first.start()

    @pl.when(home)
    def _():
        local.start()

    for load in loads:
        load.start()

    beside = t + 1 - 2 * (t % 2)
    across = (t + 2) % 4

    def arrived(s):
        remote(xbuf.at[s], xbuf.at[s], xs.at[0], xr.at[s], k, beside).wait_recv()

    @pl.when(home)
    def _():
        local.wait()

    @pl.when(jnp.logical_not(home))
    def _():
        arrived(slot)

    over = remote(xbuf.at[slot], xbuf.at[slot], xs.at[1], xr.at[slot], k, across)
    over.start()
    near = remote(xbuf.at[slot], xbuf.at[slot], xs.at[2], xr.at[slot], k, beside)
    near.start()
    other = turned_slot(across)
    arrived(other)
    onward = remote(xbuf.at[other], xbuf.at[other], xs.at[3], xr.at[other], k, beside)
    onward.start()
    arrived(turned_slot(beside))
    arrived(turned_slot((beside + 2) % 4))
    for load in loads:
        load.wait()

    def step(i, carry):
        r = pick(k, [pick(i, row) for row in ORDER])
        own = r == k
        floated = xbuf[r].astype(f32)
        gained = (floated * gain_ref[k]).astype(bf16)
        squares = floated * floated
        high = squares.astype(bf16)
        rest = (squares - high.astype(f32)).astype(bf16)
        ones = jnp.ones((8, depth), bf16)
        nt = (((1,), (1,)), ((), ()))
        esend[r, 0:16, :] = lax.dot_general(fs[0], gained, nt, preferred_element_type=f32)
        esend[r, 16:32, :] = lax.dot_general(fs[1], gained, nt, preferred_element_type=f32)
        esend[r, 32:40, :] = lax.dot_general(ones, high, nt, preferred_element_type=f32) + lax.dot_general(
            ones, rest, nt, preferred_element_type=f32
        )
        for j in range(4):
            part = jnp.dot(gained, w[j], preferred_element_type=f32)
            cols = slice(j * width, (j + 1) * width)

            @pl.when(own)
            def _():
                acc[:, cols] = part

            @pl.when(jnp.logical_not(own))
            def _():
                send[r, :, cols] = part.astype(bf16)

        relayed = jnp.logical_or(jnp.logical_and(k == 1, r == 3), jnp.logical_and(k == 2, r == 0))

        @pl.when(relayed)
        def _():
            remote(send.at[r], recv.at[4], ps.at[r], pr.at[4], k, beside).wait_recv()

            def add(c, carry):
                at_rows = pl.ds(c * 16, 16)
                send[r, at_rows, :] = (send[r, at_rows, :].astype(f32) + recv[4, at_rows, :].astype(f32)).astype(bf16)
                return carry

            lax.fori_loop(0, rows // 16, add, 0)

        @pl.when(jnp.logical_not(own))
        def _():
            ends = jnp.logical_or(jnp.logical_and(k == 0, r == 3), jnp.logical_and(k == 3, r == 0))
            target = jnp.where(ends, jnp.where(k == 0, 1, 2), r)
            place = jnp.where(ends, 4, k)
            remote(send.at[r], recv.at[place], ps.at[r], pr.at[place], target, t).start()
            remote(esend.at[r], erecv.at[k], es.at[r], er.at[k], r, t).start()

        return carry

    lax.fori_loop(0, 4, step, 0)

    first_wait = jnp.logical_not(home)

    @pl.when(first_wait)
    def _():
        first.wait_send()

    over.wait_send()
    near.wait_send()
    onward.wait_send()

    few_ref[...] = esend[k]
    for src in range(4):

        @pl.when(k != src)
        def _():
            remote(esend.at[src], erecv.at[src], es.at[src], er.at[src], k, beside).wait()
            few_ref[...] += erecv[src]
            remote(send.at[src], recv.at[src], ps.at[src], pr.at[src], k, beside).wait_send()

        @pl.when(jnp.logical_and(k != src, k + src != 3) if src in (0, 3) else k != src)
        def _():
            remote(send.at[src], recv.at[src], ps.at[src], pr.at[src], k, beside).wait_recv()

            def add(c, carry):
                at_rows = pl.ds(c * 16, 16)
                acc[at_rows, :] = acc[at_rows, :] + recv[src, at_rows, :].astype(f32)
                return carry

            lax.fori_loop(0, rows // 16, add, 0)


def project(x, gain, weights, forgetting, strength):
    rows, depth = x.shape
    width = weights[0].shape[1]
    vmem, hbm = pl.BlockSpec(memory_space=pltpu.VMEM), pl.BlockSpec(memory_space=pl.ANY)
    dma = pltpu.SemaphoreType.DMA
    return pl.pallas_call(
        project_kernel,
        in_specs=[vmem, vmem] + [hbm] * 6,
        out_specs=[vmem, vmem],
        out_shape=[jax.ShapeDtypeStruct((rows, 4 * width), f32), jax.ShapeDtypeStruct((40, rows), f32)],
        scratch_shapes=[
            pltpu.VMEM((4, rows, depth), bf16),
            pltpu.VMEM((4, depth, width), bf16),
            pltpu.VMEM((2, forgetting.shape[1], depth), bf16),
            pltpu.VMEM((4, rows, 4 * width), bf16),
            pltpu.VMEM((5, rows, 4 * width), bf16),
            pltpu.VMEM((4, 40, rows), f32),
            pltpu.VMEM((4, 40, rows), f32),
            dma((4,)), dma((4,)), dma((6,)), dma((4,)), dma((5,)), dma((4,)), dma((4,)),
        ],
        compiler_params=pltpu.CompilerParams(has_side_effects=True, vmem_limit_bytes=56 * 2**20),
        name="project",
    )(x, gain.reshape(-1, 1, depth), *weights, forgetting.T, strength.T)


NEAREST = ((0, 1, 2, 3), (1, 0, 2, 3), (2, 3, 1, 0), (3, 2, 1, 0))


def mix_kernel(flat_ref, wo, o_ref, held, w, part, mate, cross, total, wsem, gs, gr, ms, mr, xs, xr, ts, tr):
    k, t, g = lax.axis_index("kv"), lax.axis_index("tp"), lax.axis_index("grp")
    rows = flat_ref.shape[0]

    def remote(src, dst, ss, rs, kv, tp):
        return pltpu.make_async_remote_copy(
            src, dst, ss, rs, device_id={"grp": g, "kv": kv, "tp": tp}, device_id_type=pl.DeviceIdType.MESH
        )

    load = pltpu.make_async_copy(wo, w, wsem.at[0])
    own = pltpu.make_async_copy(flat_ref, held.at[k], wsem.at[1])
    own.start()
    sends = [remote(flat_ref, held.at[k], gs.at[n], gr.at[k], lax.rem(k + n, 4), t) for n in (1, 2, 3)]
    for copy in sends:
        copy.start()
    load.start()
    beside = t + 1 - 2 * (t % 2)
    across = (t + 2) % 4
    diagonal = (beside + 2) % 4
    load.wait()
    own.wait()

    def to_mate(r, n):
        return remote(part.at[r], mate.at[n], ms.at[n], mr.at[n], k, beside)

    def to_cross(r):
        return remote(part.at[r], cross, xs, xr, k, across)

    def step(i, carry):
        r = pick(k, [pick(i, row) for row in NEAREST])

        @pl.when(r != k)
        def _():
            remote(held.at[r], held.at[r], gs.at[0], gr.at[r], r, t).wait_recv()

        part[r] = jnp.dot(held[r], w[...], preferred_element_type=f32).astype(bf16)
        sink = turned_slot(r)

        @pl.when(sink == beside)
        def _():
            to_mate(r, 0).start()

        @pl.when(sink == diagonal)
        def _():
            to_mate(r, 1).start()

        @pl.when(sink == across)
        def _():
            to_mate(r, 1).wait_recv()

            def add(c, carry):
                at_rows = pl.ds(c * 16, 16)
                part[r, at_rows, :] = (part[r, at_rows, :].astype(f32) + mate[1, at_rows, :].astype(f32)).astype(bf16)
                return carry

            lax.fori_loop(0, rows // 16, add, 0)
            to_cross(r).start()

        return carry

    lax.fori_loop(0, 4, step, 0)
    mine = turned_slot(t)
    to_mate(mine, 0).wait_recv()
    to_cross(mine).wait_recv()

    def add(c, carry):
        at_rows = pl.ds(c * 16, 16)
        total[at_rows, :] = (
            part[mine, at_rows, :].astype(f32) + mate[0, at_rows, :].astype(f32) + cross[at_rows, :].astype(f32)
        ).astype(bf16)
        return carry

    lax.fori_loop(0, rows // 16, add, 0)
    home = jnp.logical_and(mine == k, t == k)
    last = remote(total, o_ref, ts, tr, mine, k)
    local = pltpu.make_async_copy(total, o_ref, tr)

    @pl.when(home)
    def _():
        local.start()
        local.wait()

    @pl.when(jnp.logical_not(home))
    def _():
        last.start()
        last.wait()

    for copy in sends:
        copy.wait_send()
    to_mate(0, 0).wait_send()
    to_mate(0, 1).wait_send()
    to_cross(0).wait_send()


def mix(flat, final):
    rows, width = flat.shape
    cols = final.shape[1]
    vmem, hbm = pl.BlockSpec(memory_space=pltpu.VMEM), pl.BlockSpec(memory_space=pl.ANY)
    dma = pltpu.SemaphoreType.DMA
    return pl.pallas_call(
        mix_kernel,
        in_specs=[vmem, hbm],
        out_specs=vmem,
        out_shape=jax.ShapeDtypeStruct((rows, cols), bf16),
        scratch_shapes=[
            pltpu.VMEM((4, rows, width), bf16),
            pltpu.VMEM((width, cols), bf16),
            pltpu.VMEM((4, rows, cols), bf16),
            pltpu.VMEM((2, rows, cols), bf16),
            pltpu.VMEM((rows, cols), bf16),
            pltpu.VMEM((rows, cols), bf16),
            dma((2,)), dma((4,)), dma((4,)), dma((2,)), dma((2,)), dma, dma, dma, dma,
        ],
        compiler_params=pltpu.CompilerParams(has_side_effects=True, vmem_limit_bytes=56 * 2**20),
        name="mix",
    )(flat, final)


def on_device(
    n_kv,
    n_tp,
    candidate_embeddings,
    incoming_rms_scaling,
    probe_projector,
    address_projector,
    content_projector,
    sigmoid_mask_matrix,
    forgetting_projector,
    strength_projector_matrix,
    channel_forgetting_rates,
    forgetting_offset,
    extra_forgetting,
    outgoing_rms_scaling,
    final_projector,
    memory_matrix,
    earlier_addresses,
    earlier_contents,
    earlier_strengths,
    earlier_forgetting,
    admitted_counts,
):
    rows, local_cols = candidate_embeddings.shape
    features = incoming_rms_scaling.shape[0]
    depth, width = probe_projector.shape
    heads = width // DK
    seqs = rows // P_SIZE
    k_index, t_index = lax.axis_index("kv"), lax.axis_index("tp")

    def thin(values):
        return values.reshape(seqs, P_SIZE * heads)

    weights = (probe_projector, address_projector, content_projector, sigmoid_mask_matrix)
    if n_kv == 4 and n_tp == 4:
        summed, few = project(
            candidate_embeddings, incoming_rms_scaling, weights, forgetting_projector, strength_projector_matrix
        )
        columns = forgetting_projector.shape[1]
        few = [lax.dynamic_slice_in_dim(few, n * columns + t_index * heads, heads) for n in range(2)] + [few[2 * columns : 2 * columns + 1]]
        few = jnp.concatenate(few, axis=0).T
    else:
        every = lax.all_gather(candidate_embeddings, "tp", axis=1, tiled=True)
        every = lax.all_to_all(every, "kv", split_axis=1, concat_axis=0, tiled=True)
        gain_part = lax.dynamic_slice_in_dim(incoming_rms_scaling, k_index * depth, depth)
        floated = every.astype(f32)
        gained = (floated * gain_part).astype(bf16)
        decay_cols = lax.dynamic_slice(forgetting_projector, (k_index * depth, t_index * heads), (depth, heads))
        beta_cols = lax.dynamic_slice(strength_projector_matrix, (k_index * depth, t_index * heads), (depth, heads))
        few = jnp.concatenate(
            [
                jnp.dot(gained, jnp.concatenate([decay_cols, beta_cols], axis=1), preferred_element_type=f32),
                jnp.sum(floated * floated, axis=1, keepdims=True),
            ],
            axis=1,
        )
        few = lax.psum_scatter(few, "kv", scatter_dimension=0, tiled=True)
        partial = jnp.concatenate(
            [jnp.dot(gained, w, preferred_element_type=f32).astype(bf16) for w in weights], axis=1
        )
        summed = lax.psum_scatter(partial, "kv", scatter_dimension=0, tiled=True).astype(f32)
    taken = accepted(
        memory_matrix,
        earlier_addresses.reshape(rows, width),
        earlier_contents.reshape(rows, width),
        jnp.concatenate(
            [thin(earlier_forgetting), thin(earlier_strengths), admitted_counts.astype(f32).reshape(seqs, 1)], axis=1
        ),
    )
    factor = lax.rsqrt(few[:, 2 * heads :] / features + epsilon)
    few = few[:, : 2 * heads] * factor
    decay_in = few[:, :heads].reshape(seqs, P_SIZE, heads)
    beta = jax.nn.sigmoid(few[:, heads:].reshape(seqs, P_SIZE, heads))
    decay = -jnp.exp(channel_forgetting_rates) * jax.nn.softplus(decay_in + forgetting_offset) + extra_forgetting
    flat = attend(taken, summed, factor, thin(decay), thin(beta), outgoing_rms_scaling)
    if n_kv == 4 and n_tp == 4:
        mixed = mix(flat, final_projector)
    else:
        gathered = lax.all_gather(flat, "kv", axis=0, tiled=True)
        terms = jnp.dot(gathered, final_projector, preferred_element_type=f32).astype(bf16)
        terms = lax.all_to_all(terms, "kv", split_axis=0, concat_axis=1, tiled=True)
        mixed = lax.psum_scatter(terms, "tp", scatter_dimension=1, tiled=True)
    return (mixed, taken)


def solution(mesh):
    row, per_head = P(("grp", "kv"), "tp"), P(("grp", "kv"), None, "tp")
    four = P(("grp", "kv"), None, "tp", None)
    weight = P("kv", "tp")
    state = P(("grp", "kv"), "tp", None, None)
    in_specs = (
        row, P(), weight, weight, weight, weight, P(), P(), P("tp"), P("tp"), per_head, P(),
        P("tp", "kv"), state, four, four, per_head, per_head, P(("grp", "kv")),
    )
    body = functools.partial(on_device, mesh.shape["kv"], mesh.shape["tp"])
    return jax.shard_map(body, mesh=mesh, in_specs=in_specs, out_specs=(row, state), check_vma=False)
```

```python
import functools

import jax
import jax.numpy as jnp
from jax import lax
from jax.experimental import pallas as pl
from jax.experimental.pallas import tpu as pltpu
from jax.sharding import PartitionSpec as P

DK = 128
P_SIZE = 4
SB = 8
TALL = SB * P_SIZE
epsilon = 1e-06
f32 = jnp.float32
bf16 = jnp.bfloat16


def lane_dot(a, b):
    return jnp.sum(a * b, axis=-1, keepdims=True)


def first_half():
    return lax.broadcasted_iota(jnp.int32, (8, DK), 0) < P_SIZE


def load_heads(heads, src, dst, factor=None):
    for h in range(heads):
        part = src[:, h * DK : (h + 1) * DK].astype(f32)
        dst[pl.ds(h * TALL, TALL), :] = part if factor is None else (part * factor).astype(bf16).astype(f32)


def tile(h, pair):
    return pl.ds(h * TALL + pair * 8, 8)


def proposal(h, p):
    return pl.ds(h * TALL + p, SB, stride=P_SIZE)


def accepted_kernel(heads, s_ref, k_ref, v_ref, n_ref, o_ref, r_scr, u_scr, c_scr, kf, vf):
    load_heads(heads, k_ref, kf)
    load_heads(heads, v_ref, vf)
    low = first_half()
    for pair in range(SB // 2):
        for h in range(heads):
            at = tile(h, pair)
            lhs = kf[at, :].astype(bf16)
            r0 = jnp.dot(lhs, s_ref[2 * pair, h].astype(bf16), preferred_element_type=f32)
            r1 = jnp.dot(lhs, s_ref[2 * pair + 1, h].astype(bf16), preferred_element_type=f32)
            r_scr[at, :] = jnp.where(low, r0, r1)
    few = n_ref[...]
    span = P_SIZE * heads
    count = few[:, 2 * span : 2 * span + 1]
    for h in range(heads):
        scale = jnp.ones((SB, 1), f32)
        ks, us, norms = [], [], []
        for p in range(P_SIZE):
            at = proposal(h, p)
            col = slice(p * heads + h, p * heads + h + 1)
            key = kf[at, :]
            norm = lax.rsqrt(lane_dot(key, key) + epsilon)
            live = count > float(p)
            g = jnp.where(live, jnp.exp(few[:, p * heads + h : p * heads + h + 1]), 1.0)
            b = jnp.where(live, few[:, span + p * heads + h : span + p * heads + h + 1], 0.0)
            rec = (scale * norm) * r_scr[at, :]
            for ki, ui, ni in zip(ks, us, norms):
                rec = rec + (lane_dot(ki, key) * (ni * norm)) * ui
            us = [ui * g for ui in us]
            scale = scale * g
            us.append(b * (vf[at, :] - g * rec))
            ks.append(key)
            norms.append(norm)
        for p in range(P_SIZE):
            u_scr[proposal(h, p), :] = us[p] * norms[p]
        c_scr[pl.ds(h * SB, SB), :] = jnp.broadcast_to(scale, (SB, DK))
    for pair in range(SB // 2):
        for h in range(heads):
            at = tile(h, pair)
            key = kf[at, :]
            lhs = jnp.concatenate([key, key], axis=0).astype(bf16)
            u = u_scr[at, :]
            hi = u.astype(bf16).astype(f32)
            lo = u - hi
            for half in range(2):
                keep = low if half == 0 else jnp.logical_not(low)
                rhs = jnp.concatenate([jnp.where(keep, hi, 0.0), jnp.where(keep, lo, 0.0)], axis=0).astype(bf16)
                seq = 2 * pair + half
                add = lax.dot_general(lhs, rhs, (((0,), (0,)), ((), ())), preferred_element_type=f32)
                o_ref[seq, h] = c_scr[pl.ds(h * SB + seq, 1), :] * s_ref[seq, h] + add


def attend_kernel(heads, s_ref, a_ref, q_ref, k_ref, v_ref, z_ref, d_ref, b_ref, w_ref, o_ref, kept, rk, rq, qf, kf, vf, zf, of, done):
    keep = pltpu.make_async_copy(s_ref, kept.at[pl.ds(pl.program_id(0) * SB, SB)], done)
    keep.start()
    for src, dst in ((q_ref, qf), (k_ref, kf), (v_ref, vf), (z_ref, zf)):
        load_heads(heads, src, dst, a_ref[...])
    low = first_half()
    for pair in range(SB // 2):
        for h in range(heads):
            at = tile(h, pair)
            lhs = jnp.concatenate([kf[at, :], qf[at, :]], axis=0).astype(bf16)
            r0 = jnp.dot(lhs, s_ref[2 * pair, h].astype(bf16), preferred_element_type=f32)
            r1 = jnp.dot(lhs, s_ref[2 * pair + 1, h].astype(bf16), preferred_element_type=f32)
            rk[at, :] = jnp.where(low, r0[:8], r1[:8])
            rq[at, :] = jnp.where(low, r0[8:], r1[8:])
    gain = w_ref[...]
    for h in range(heads):
        scale = jnp.ones((SB, 1), f32)
        ks, us, norms = [], [], []
        for p in range(P_SIZE):
            at = proposal(h, p)
            col = slice(p * heads + h, p * heads + h + 1)
            key = kf[at, :]
            query = qf[at, :]
            norm = lax.rsqrt(lane_dot(key, key) + epsilon)
            qnorm = lax.rsqrt(lane_dot(query, query) + epsilon) * DK ** (-0.5)
            g = jnp.exp(d_ref[:, col])
            rec = (scale * norm) * rk[at, :]
            for ki, ui, ni in zip(ks, us, norms):
                rec = rec + (lane_dot(ki, key) * (ni * norm)) * ui
            us = [ui * g for ui in us]
            scale = scale * g
            us.append(b_ref[:, col] * (vf[at, :] - g * rec))
            ks.append(key)
            norms.append(norm)
            att = (scale * qnorm) * rq[at, :]
            for ki, ui, ni in zip(ks, us, norms):
                att = att + (lane_dot(ki, query) * (ni * qnorm)) * ui
            gate = zf[at, :]
            mean = jnp.sum(att * att, axis=-1, keepdims=True) / DK
            of[at, :] = att * lax.rsqrt(mean + epsilon) * gain * (gate * jax.nn.sigmoid(gate))
    for h in range(heads):
        o_ref[:, h * DK : (h + 1) * DK] = of[pl.ds(h * TALL, TALL), :].astype(bf16)
    keep.wait()


def accepted(state, keys, values, few):
    seqs, heads = state.shape[:2]
    width = heads * DK
    rows = TALL
    tall = pl.BlockSpec((rows, width), lambda i: (i, 0))
    thin = pl.BlockSpec((SB, few.shape[1]), lambda i: (i, 0))
    block = pl.BlockSpec((SB, heads, DK, DK), lambda i: (i, 0, 0, 0))
    return pl.pallas_call(
        functools.partial(accepted_kernel, heads),
        grid=(seqs // SB,),
        in_specs=[block, tall, tall, thin],
        out_specs=block,
        out_shape=jax.ShapeDtypeStruct(state.shape, f32),
        scratch_shapes=[pltpu.VMEM((heads * n, DK), f32) for n in (TALL, TALL, SB, TALL, TALL)],
        cost_estimate=pl.CostEstimate(flops=10_000_000_000, bytes_accessed=2 * state.size * 4, transcendentals=0),
        name="accepted",
    )(state, keys, values, few)


def attend(state, packed, factor, decay, beta, gain):
    seqs, heads = state.shape[:2]
    width = heads * DK
    rows = TALL
    thin = pl.BlockSpec((SB, P_SIZE * heads), lambda i: (i, 0))
    block = pl.BlockSpec((SB, heads, DK, DK), lambda i: (i, 0, 0, 0))

    def part(n):
        return pl.BlockSpec((rows, width), lambda i: (i, n))

    return pl.pallas_call(
        functools.partial(attend_kernel, heads),
        grid=(seqs // SB,),
        in_specs=[block, pl.BlockSpec((rows, 1), lambda i: (i, 0)), part(0), part(1), part(2), part(3), thin, thin, pl.BlockSpec((1, DK), lambda i: (0, 0))],
        out_specs=[pl.BlockSpec((rows, width), lambda i: (i, 0)), pl.BlockSpec(memory_space=pl.ANY)],
        out_shape=[jax.ShapeDtypeStruct((seqs * P_SIZE, width), bf16), jax.ShapeDtypeStruct(state.shape, f32)],
        scratch_shapes=[pltpu.VMEM((heads * TALL, DK), f32)] * 7 + [pltpu.SemaphoreType.DMA],
        cost_estimate=pl.CostEstimate(flops=5_000_000_000, bytes_accessed=state.size * 4, transcendentals=0),
        name="attend",
    )(state, factor, packed, packed, packed, packed, decay, beta, gain.reshape(1, DK))


def pick(index, values):
    chosen = values[-1]
    for at, value in enumerate(values[:-1]):
        chosen = jnp.where(index == at, value, chosen)
    return chosen


def turned_slot(t):
    return pick(t, (0, 2, 1, 3))


ORDER = ((3, 2, 1, 0), (0, 2, 1, 3), (3, 1, 2, 0), (0, 1, 2, 3))


def project_kernel(x_ref, gain_ref, keys, values, thin, wq, wk, wv, wz, wf, ws, state, acc, few_ref, taken, xbuf, w, fs,
                   send, recv, esend, erecv, s_in, s_out, r_scr, u_scr, c_scr, kf, vf,
                   xs, xr, wsem, ps, pr, es, er, ins, outs):
    k, t, g = lax.axis_index("kv"), lax.axis_index("tp"), lax.axis_index("grp")
    depth, width = w.shape[1], w.shape[2]
    rows = x_ref.shape[0]

    def at(kv, tp):
        return {"grp": g, "kv": kv, "tp": tp}

    def remote(src, dst, ss, rs, kv, tp):
        return pltpu.make_async_remote_copy(src, dst, ss, rs, device_id=at(kv, tp), device_id_type=pl.DeviceIdType.MESH)

    loads = [pltpu.make_async_copy(src, w.at[i], wsem.at[i]) for i, src in enumerate((wq, wk, wv, wz))]
    here = pl.ds(k * depth, depth)
    loads += [pltpu.make_async_copy(src.at[:, here], fs.at[i], wsem.at[4 + i]) for i, src in enumerate((wf, ws))]
    slot = turned_slot(t)
    far_t, far_k = turned_slot(k), t
    home = jnp.logical_and(far_k == k, far_t == t)
    first = remote(x_ref, xbuf.at[k], xs.at[0], xr.at[k], far_k, far_t)
    local = pltpu.make_async_copy(x_ref, xbuf.at[k], xr.at[k])

    @pl.when(jnp.logical_not(home))
    def _():
        first.start()

    @pl.when(home)
    def _():
        local.start()

    for load in loads:
        load.start()

    beside = t + 1 - 2 * (t % 2)
    across = (t + 2) % 4

    def arrived(s):
        remote(xbuf.at[s], xbuf.at[s], xs.at[0], xr.at[s], k, beside).wait_recv()

    @pl.when(home)
    def _():
        local.wait()

    @pl.when(jnp.logical_not(home))
    def _():
        arrived(slot)

    over = remote(xbuf.at[slot], xbuf.at[slot], xs.at[1], xr.at[slot], k, across)
    over.start()
    near = remote(xbuf.at[slot], xbuf.at[slot], xs.at[2], xr.at[slot], k, beside)
    near.start()
    other = turned_slot(across)
    arrived(other)
    onward = remote(xbuf.at[other], xbuf.at[other], xs.at[3], xr.at[other], k, beside)
    onward.start()
    arrived(turned_slot(beside))
    arrived(turned_slot((beside + 2) % 4))
    for load in loads:
        load.wait()

    def step(i, carry):
        r = pick(k, [pick(i, row) for row in ORDER])
        own = r == k
        floated = xbuf[r].astype(f32)
        gained = (floated * gain_ref[k]).astype(bf16)
        squares = floated * floated
        high = squares.astype(bf16)
        rest = (squares - high.astype(f32)).astype(bf16)
        ones = jnp.ones((8, depth), bf16)
        nt = (((1,), (1,)), ((), ()))
        esend[r, 0:16, :] = lax.dot_general(fs[0], gained, nt, preferred_element_type=f32)
        esend[r, 16:32, :] = lax.dot_general(fs[1], gained, nt, preferred_element_type=f32)
        esend[r, 32:40, :] = lax.dot_general(ones, high, nt, preferred_element_type=f32) + lax.dot_general(
            ones, rest, nt, preferred_element_type=f32
        )
        for j in range(4):
            part = jnp.dot(gained, w[j], preferred_element_type=f32)
            cols = slice(j * width, (j + 1) * width)

            @pl.when(own)
            def _():
                acc[:, cols] = part

            @pl.when(jnp.logical_not(own))
            def _():
                send[r, :, cols] = part.astype(bf16)

        relayed = jnp.logical_or(jnp.logical_and(k == 1, r == 3), jnp.logical_and(k == 2, r == 0))

        @pl.when(relayed)
        def _():
            remote(send.at[r], recv.at[4], ps.at[r], pr.at[4], k, beside).wait_recv()

            def add(c, carry):
                at_rows = pl.ds(c * 16, 16)
                send[r, at_rows, :] = (send[r, at_rows, :].astype(f32) + recv[4, at_rows, :].astype(f32)).astype(bf16)
                return carry

            lax.fori_loop(0, rows // 16, add, 0)

        @pl.when(jnp.logical_not(own))
        def _():
            ends = jnp.logical_or(jnp.logical_and(k == 0, r == 3), jnp.logical_and(k == 3, r == 0))
            target = jnp.where(ends, jnp.where(k == 0, 1, 2), r)
            place = jnp.where(ends, 4, k)
            remote(send.at[r], recv.at[place], ps.at[r], pr.at[place], target, t).start()
            remote(esend.at[r], erecv.at[k], es.at[r], er.at[k], r, t).start()

        return carry

    lax.fori_loop(0, 3, step, 0)

    blocks = state.shape[0] // SB
    heads = state.shape[1]

    def fetch(i):
        return pltpu.make_async_copy(state.at[pl.ds(i * SB, SB)], s_in.at[i % 2], ins.at[i % 2])

    def put(i):
        return pltpu.make_async_copy(s_out.at[i % 2], taken.at[pl.ds(i * SB, SB)], outs.at[i % 2])

    def accept(i, carry):
        @pl.when(i + 1 < blocks)
        def _():
            fetch(i + 1).start()

        fetch(i).wait()

        @pl.when(i >= 2)
        def _():
            put(i - 2).wait()

        tall, few_rows = pl.ds(i * TALL, TALL), pl.ds(i * SB, SB)
        accepted_kernel(
            heads, s_in.at[i % 2], keys.at[tall], values.at[tall], thin.at[few_rows], s_out.at[i % 2],
            r_scr, u_scr, c_scr, kf, vf,
        )
        put(i).start()
        return carry

    fetch(0).start()
    lax.fori_loop(0, blocks, accept, 0)
    lax.fori_loop(3, 4, step, 0)
    for i in range(max(blocks - 2, 0), blocks):
        put(i).wait()

    first_wait = jnp.logical_not(home)

    @pl.when(first_wait)
    def _():
        first.wait_send()

    over.wait_send()
    near.wait_send()
    onward.wait_send()

    few_ref[...] = esend[k]
    for src in range(4):

        @pl.when(k != src)
        def _():
            remote(esend.at[src], erecv.at[src], es.at[src], er.at[src], k, beside).wait()
            few_ref[...] += erecv[src]
            remote(send.at[src], recv.at[src], ps.at[src], pr.at[src], k, beside).wait_send()

        @pl.when(jnp.logical_and(k != src, k + src != 3) if src in (0, 3) else k != src)
        def _():
            remote(send.at[src], recv.at[src], ps.at[src], pr.at[src], k, beside).wait_recv()

            def add(c, carry):
                at_rows = pl.ds(c * 16, 16)
                acc[at_rows, :] = acc[at_rows, :] + recv[src, at_rows, :].astype(f32)
                return carry

            lax.fori_loop(0, rows // 16, add, 0)


def project(x, gain, weights, forgetting, strength, state, keys, values, thin):
    rows, depth = x.shape
    width = weights[0].shape[1]
    vmem, hbm = pl.BlockSpec(memory_space=pltpu.VMEM), pl.BlockSpec(memory_space=pl.ANY)
    dma = pltpu.SemaphoreType.DMA
    heads = state.shape[1]
    return pl.pallas_call(
        project_kernel,
        in_specs=[vmem] * 5 + [hbm] * 7,
        out_specs=[vmem, vmem, hbm],
        out_shape=[
            jax.ShapeDtypeStruct((rows, 4 * width), f32),
            jax.ShapeDtypeStruct((40, rows), f32),
            jax.ShapeDtypeStruct(state.shape, f32),
        ],
        scratch_shapes=[
            pltpu.VMEM((4, rows, depth), bf16),
            pltpu.VMEM((4, depth, width), bf16),
            pltpu.VMEM((2, forgetting.shape[1], depth), bf16),
            pltpu.VMEM((4, rows, 4 * width), bf16),
            pltpu.VMEM((5, rows, 4 * width), bf16),
            pltpu.VMEM((4, 40, rows), f32),
            pltpu.VMEM((4, 40, rows), f32),
            pltpu.VMEM((2, SB) + state.shape[1:], f32),
            pltpu.VMEM((2, SB) + state.shape[1:], f32),
            *[pltpu.VMEM((heads * n, DK), f32) for n in (TALL, TALL, SB, TALL, TALL)],
            dma((4,)), dma((4,)), dma((6,)), dma((4,)), dma((5,)), dma((4,)), dma((4,)), dma((2,)), dma((2,)),
        ],
        compiler_params=pltpu.CompilerParams(has_side_effects=True, vmem_limit_bytes=56 * 2**20),
        name="project",
    )(x, gain.reshape(-1, 1, depth), keys, values, thin, *weights, forgetting.T, strength.T, state)


NEAREST = ((0, 1, 2, 3), (1, 0, 2, 3), (2, 3, 1, 0), (3, 2, 1, 0))


def mix_kernel(flat_ref, wo, o_ref, held, w, part, mate, cross, total, wsem, gs, gr, ms, mr, xs, xr, ts, tr):
    k, t, g = lax.axis_index("kv"), lax.axis_index("tp"), lax.axis_index("grp")
    rows = flat_ref.shape[0]

    def remote(src, dst, ss, rs, kv, tp):
        return pltpu.make_async_remote_copy(
            src, dst, ss, rs, device_id={"grp": g, "kv": kv, "tp": tp}, device_id_type=pl.DeviceIdType.MESH
        )

    load = pltpu.make_async_copy(wo, w, wsem.at[0])
    own = pltpu.make_async_copy(flat_ref, held.at[k], wsem.at[1])
    own.start()
    sends = [remote(flat_ref, held.at[k], gs.at[n], gr.at[k], lax.rem(k + n, 4), t) for n in (1, 2, 3)]
    for copy in sends:
        copy.start()
    load.start()
    beside = t + 1 - 2 * (t % 2)
    across = (t + 2) % 4
    diagonal = (beside + 2) % 4
    load.wait()
    own.wait()

    def to_mate(r, n):
        return remote(part.at[r], mate.at[n], ms.at[n], mr.at[n], k, beside)

    def to_cross(r):
        return remote(part.at[r], cross, xs, xr, k, across)

    def step(i, carry):
        r = pick(k, [pick(i, row) for row in NEAREST])

        @pl.when(r != k)
        def _():
            remote(held.at[r], held.at[r], gs.at[0], gr.at[r], r, t).wait_recv()

        part[r] = jnp.dot(held[r], w[...], preferred_element_type=f32).astype(bf16)
        sink = turned_slot(r)

        @pl.when(sink == beside)
        def _():
            to_mate(r, 0).start()

        @pl.when(sink == diagonal)
        def _():
            to_mate(r, 1).start()

        @pl.when(sink == across)
        def _():
            to_mate(r, 1).wait_recv()

            def add(c, carry):
                at_rows = pl.ds(c * 16, 16)
                part[r, at_rows, :] = (part[r, at_rows, :].astype(f32) + mate[1, at_rows, :].astype(f32)).astype(bf16)
                return carry

            lax.fori_loop(0, rows // 16, add, 0)
            to_cross(r).start()

        return carry

    lax.fori_loop(0, 4, step, 0)
    mine = turned_slot(t)
    to_mate(mine, 0).wait_recv()
    to_cross(mine).wait_recv()

    def add(c, carry):
        at_rows = pl.ds(c * 16, 16)
        total[at_rows, :] = (
            part[mine, at_rows, :].astype(f32) + mate[0, at_rows, :].astype(f32) + cross[at_rows, :].astype(f32)
        ).astype(bf16)
        return carry

    lax.fori_loop(0, rows // 16, add, 0)
    home = jnp.logical_and(mine == k, t == k)
    last = remote(total, o_ref, ts, tr, mine, k)
    local = pltpu.make_async_copy(total, o_ref, tr)

    @pl.when(home)
    def _():
        local.start()
        local.wait()

    @pl.when(jnp.logical_not(home))
    def _():
        last.start()
        last.wait()

    for copy in sends:
        copy.wait_send()
    to_mate(0, 0).wait_send()
    to_mate(0, 1).wait_send()
    to_cross(0).wait_send()


def mix(flat, final):
    rows, width = flat.shape
    cols = final.shape[1]
    vmem, hbm = pl.BlockSpec(memory_space=pltpu.VMEM), pl.BlockSpec(memory_space=pl.ANY)
    dma = pltpu.SemaphoreType.DMA
    return pl.pallas_call(
        mix_kernel,
        in_specs=[vmem, hbm],
        out_specs=vmem,
        out_shape=jax.ShapeDtypeStruct((rows, cols), bf16),
        scratch_shapes=[
            pltpu.VMEM((4, rows, width), bf16),
            pltpu.VMEM((width, cols), bf16),
            pltpu.VMEM((4, rows, cols), bf16),
            pltpu.VMEM((2, rows, cols), bf16),
            pltpu.VMEM((rows, cols), bf16),
            pltpu.VMEM((rows, cols), bf16),
            dma((2,)), dma((4,)), dma((4,)), dma((2,)), dma((2,)), dma, dma, dma, dma,
        ],
        compiler_params=pltpu.CompilerParams(has_side_effects=True, vmem_limit_bytes=56 * 2**20),
        name="mix",
    )(flat, final)


def on_device(
    n_kv,
    n_tp,
    candidate_embeddings,
    incoming_rms_scaling,
    probe_projector,
    address_projector,
    content_projector,
    sigmoid_mask_matrix,
    forgetting_projector,
    strength_projector_matrix,
    channel_forgetting_rates,
    forgetting_offset,
    extra_forgetting,
    outgoing_rms_scaling,
    final_projector,
    memory_matrix,
    earlier_addresses,
    earlier_contents,
    earlier_strengths,
    earlier_forgetting,
    admitted_counts,
):
    rows, local_cols = candidate_embeddings.shape
    features = incoming_rms_scaling.shape[0]
    depth, width = probe_projector.shape
    heads = width // DK
    seqs = rows // P_SIZE
    k_index, t_index = lax.axis_index("kv"), lax.axis_index("tp")

    def thin(values):
        return values.reshape(seqs, P_SIZE * heads)

    weights = (probe_projector, address_projector, content_projector, sigmoid_mask_matrix)
    earlier = (
        memory_matrix,
        earlier_addresses.reshape(rows, width),
        earlier_contents.reshape(rows, width),
        jnp.concatenate(
            [thin(earlier_forgetting), thin(earlier_strengths), admitted_counts.astype(f32).reshape(seqs, 1)], axis=1
        ),
    )
    if n_kv == 4 and n_tp == 4:
        summed, few, taken = project(
            candidate_embeddings, incoming_rms_scaling, weights, forgetting_projector, strength_projector_matrix, *earlier
        )
        columns = forgetting_projector.shape[1]
        few = [lax.dynamic_slice_in_dim(few, n * columns + t_index * heads, heads) for n in range(2)] + [few[2 * columns : 2 * columns + 1]]
        few = jnp.concatenate(few, axis=0).T
    else:
        every = lax.all_gather(candidate_embeddings, "tp", axis=1, tiled=True)
        every = lax.all_to_all(every, "kv", split_axis=1, concat_axis=0, tiled=True)
        gain_part = lax.dynamic_slice_in_dim(incoming_rms_scaling, k_index * depth, depth)
        floated = every.astype(f32)
        gained = (floated * gain_part).astype(bf16)
        decay_cols = lax.dynamic_slice(forgetting_projector, (k_index * depth, t_index * heads), (depth, heads))
        beta_cols = lax.dynamic_slice(strength_projector_matrix, (k_index * depth, t_index * heads), (depth, heads))
        few = jnp.concatenate(
            [
                jnp.dot(gained, jnp.concatenate([decay_cols, beta_cols], axis=1), preferred_element_type=f32),
                jnp.sum(floated * floated, axis=1, keepdims=True),
            ],
            axis=1,
        )
        few = lax.psum_scatter(few, "kv", scatter_dimension=0, tiled=True)
        partial = jnp.concatenate(
            [jnp.dot(gained, w, preferred_element_type=f32).astype(bf16) for w in weights], axis=1
        )
        summed = lax.psum_scatter(partial, "kv", scatter_dimension=0, tiled=True).astype(f32)
        taken = accepted(*earlier)
    factor = lax.rsqrt(few[:, 2 * heads :] / features + epsilon)
    few = few[:, : 2 * heads] * factor
    decay_in = few[:, :heads].reshape(seqs, P_SIZE, heads)
    beta = jax.nn.sigmoid(few[:, heads:].reshape(seqs, P_SIZE, heads))
    decay = -jnp.exp(channel_forgetting_rates) * jax.nn.softplus(decay_in + forgetting_offset) + extra_forgetting
    flat, taken = attend(taken, summed, factor, thin(decay), thin(beta), outgoing_rms_scaling)
    if n_kv == 4 and n_tp == 4:
        mixed = mix(flat, final_projector)
    else:
        gathered = lax.all_gather(flat, "kv", axis=0, tiled=True)
        terms = jnp.dot(gathered, final_projector, preferred_element_type=f32).astype(bf16)
        terms = lax.all_to_all(terms, "kv", split_axis=0, concat_axis=1, tiled=True)
        mixed = lax.psum_scatter(terms, "tp", scatter_dimension=1, tiled=True)
    return (mixed, taken)


def solution(mesh):
    row, per_head = P(("grp", "kv"), "tp"), P(("grp", "kv"), None, "tp")
    four = P(("grp", "kv"), None, "tp", None)
    weight = P("kv", "tp")
    state = P(("grp", "kv"), "tp", None, None)
    in_specs = (
        row, P(), weight, weight, weight, weight, P(), P(), P("tp"), P("tp"), per_head, P(),
        P("tp", "kv"), state, four, four, per_head, per_head, P(("grp", "kv")),
    )
    body = functools.partial(on_device, mesh.shape["kv"], mesh.shape["tp"])
    return jax.shard_map(body, mesh=mesh, in_specs=in_specs, out_specs=(row, state), check_vma=False)
```

```python
import functools

import jax
import jax.numpy as jnp
from jax import lax
from jax.experimental import pallas as pl
from jax.experimental.pallas import tpu as pltpu
from jax.sharding import PartitionSpec as P

DK = 128
P_SIZE = 4
SB = 8
TALL = SB * P_SIZE
epsilon = 1e-06
f32 = jnp.float32
bf16 = jnp.bfloat16


def lane_dot(a, b):
    return jnp.sum(a * b, axis=-1, keepdims=True)


def first_half():
    return lax.broadcasted_iota(jnp.int32, (8, DK), 0) < P_SIZE


def load_heads(heads, src, dst, factor=None):
    for h in range(heads):
        part = src[:, h * DK : (h + 1) * DK].astype(f32)
        dst[pl.ds(h * TALL, TALL), :] = part if factor is None else (part * factor).astype(bf16).astype(f32)


def tile(h, pair):
    return pl.ds(h * TALL + pair * 8, 8)


def proposal(h, p):
    return pl.ds(h * TALL + p, SB, stride=P_SIZE)


def accepted_kernel(heads, s_ref, k_ref, v_ref, n_ref, o_ref, r_scr, u_scr, c_scr, kf, vf):
    load_heads(heads, k_ref, kf)
    load_heads(heads, v_ref, vf)
    low = first_half()
    for pair in range(SB // 2):
        for h in range(heads):
            at = tile(h, pair)
            lhs = kf[at, :].astype(bf16)
            r0 = jnp.dot(lhs, s_ref[2 * pair, h].astype(bf16), preferred_element_type=f32)
            r1 = jnp.dot(lhs, s_ref[2 * pair + 1, h].astype(bf16), preferred_element_type=f32)
            r_scr[at, :] = jnp.where(low, r0, r1)
    few = n_ref[...]
    span = P_SIZE * heads
    count = few[:, 2 * span : 2 * span + 1]
    for h in range(heads):
        scale = jnp.ones((SB, 1), f32)
        ks, us, norms = [], [], []
        for p in range(P_SIZE):
            at = proposal(h, p)
            col = slice(p * heads + h, p * heads + h + 1)
            key = kf[at, :]
            norm = lax.rsqrt(lane_dot(key, key) + epsilon)
            live = count > float(p)
            g = jnp.where(live, jnp.exp(few[:, p * heads + h : p * heads + h + 1]), 1.0)
            b = jnp.where(live, few[:, span + p * heads + h : span + p * heads + h + 1], 0.0)
            rec = (scale * norm) * r_scr[at, :]
            for ki, ui, ni in zip(ks, us, norms):
                rec = rec + (lane_dot(ki, key) * (ni * norm)) * ui
            us = [ui * g for ui in us]
            scale = scale * g
            us.append(b * (vf[at, :] - g * rec))
            ks.append(key)
            norms.append(norm)
        for p in range(P_SIZE):
            u_scr[proposal(h, p), :] = us[p] * norms[p]
        c_scr[pl.ds(h * SB, SB), :] = jnp.broadcast_to(scale, (SB, DK))
    for pair in range(SB // 2):
        for h in range(heads):
            at = tile(h, pair)
            key = kf[at, :]
            lhs = jnp.concatenate([key, key], axis=0).astype(bf16)
            u = u_scr[at, :]
            hi = u.astype(bf16).astype(f32)
            lo = u - hi
            for half in range(2):
                keep = low if half == 0 else jnp.logical_not(low)
                rhs = jnp.concatenate([jnp.where(keep, hi, 0.0), jnp.where(keep, lo, 0.0)], axis=0).astype(bf16)
                seq = 2 * pair + half
                add = lax.dot_general(lhs, rhs, (((0,), (0,)), ((), ())), preferred_element_type=f32)
                o_ref[seq, h] = c_scr[pl.ds(h * SB + seq, 1), :] * s_ref[seq, h] + add


def attend_kernel(heads, s_ref, a_ref, q_ref, k_ref, v_ref, z_ref, d_ref, b_ref, w_ref, o_ref, kept, rk, rq, qf, kf, vf, zf, of, done):
    keep = pltpu.make_async_copy(s_ref, kept.at[pl.ds(pl.program_id(0) * SB, SB)], done)
    keep.start()
    for src, dst in ((q_ref, qf), (k_ref, kf), (v_ref, vf), (z_ref, zf)):
        load_heads(heads, src, dst, a_ref[...])
    low = first_half()
    for pair in range(SB // 2):
        for h in range(heads):
            at = tile(h, pair)
            lhs = jnp.concatenate([kf[at, :], qf[at, :]], axis=0).astype(bf16)
            r0 = jnp.dot(lhs, s_ref[2 * pair, h].astype(bf16), preferred_element_type=f32)
            r1 = jnp.dot(lhs, s_ref[2 * pair + 1, h].astype(bf16), preferred_element_type=f32)
            rk[at, :] = jnp.where(low, r0[:8], r1[:8])
            rq[at, :] = jnp.where(low, r0[8:], r1[8:])
    gain = w_ref[...]
    for h in range(heads):
        scale = jnp.ones((SB, 1), f32)
        ks, us, norms = [], [], []
        for p in range(P_SIZE):
            at = proposal(h, p)
            col = slice(p * heads + h, p * heads + h + 1)
            key = kf[at, :]
            query = qf[at, :]
            norm = lax.rsqrt(lane_dot(key, key) + epsilon)
            qnorm = lax.rsqrt(lane_dot(query, query) + epsilon) * DK ** (-0.5)
            g = jnp.exp(d_ref[:, col])
            rec = (scale * norm) * rk[at, :]
            for ki, ui, ni in zip(ks, us, norms):
                rec = rec + (lane_dot(ki, key) * (ni * norm)) * ui
            us = [ui * g for ui in us]
            scale = scale * g
            us.append(b_ref[:, col] * (vf[at, :] - g * rec))
            ks.append(key)
            norms.append(norm)
            att = (scale * qnorm) * rq[at, :]
            for ki, ui, ni in zip(ks, us, norms):
                att = att + (lane_dot(ki, query) * (ni * qnorm)) * ui
            gate = zf[at, :]
            mean = jnp.sum(att * att, axis=-1, keepdims=True) / DK
            of[at, :] = att * lax.rsqrt(mean + epsilon) * gain * (gate * jax.nn.sigmoid(gate))
    for h in range(heads):
        o_ref[:, h * DK : (h + 1) * DK] = of[pl.ds(h * TALL, TALL), :].astype(bf16)
    keep.wait()


def accepted(state, keys, values, few):
    seqs, heads = state.shape[:2]
    width = heads * DK
    rows = TALL
    tall = pl.BlockSpec((rows, width), lambda i: (i, 0))
    thin = pl.BlockSpec((SB, few.shape[1]), lambda i: (i, 0))
    block = pl.BlockSpec((SB, heads, DK, DK), lambda i: (i, 0, 0, 0))
    return pl.pallas_call(
        functools.partial(accepted_kernel, heads),
        grid=(seqs // SB,),
        in_specs=[block, tall, tall, thin],
        out_specs=block,
        out_shape=jax.ShapeDtypeStruct(state.shape, f32),
        scratch_shapes=[pltpu.VMEM((heads * n, DK), f32) for n in (TALL, TALL, SB, TALL, TALL)],
        cost_estimate=pl.CostEstimate(flops=10_000_000_000, bytes_accessed=2 * state.size * 4, transcendentals=0),
        name="accepted",
    )(state, keys, values, few)


def attend(state, packed, factor, decay, beta, gain):
    seqs, heads = state.shape[:2]
    width = heads * DK
    rows = TALL
    thin = pl.BlockSpec((SB, P_SIZE * heads), lambda i: (i, 0))
    block = pl.BlockSpec((SB, heads, DK, DK), lambda i: (i, 0, 0, 0))

    def part(n):
        return pl.BlockSpec((rows, width), lambda i: (i, n))

    return pl.pallas_call(
        functools.partial(attend_kernel, heads),
        grid=(seqs // SB,),
        in_specs=[block, pl.BlockSpec((rows, 1), lambda i: (i, 0)), part(0), part(1), part(2), part(3), thin, thin, pl.BlockSpec((1, DK), lambda i: (0, 0))],
        out_specs=[pl.BlockSpec((rows, width), lambda i: (i, 0)), pl.BlockSpec(memory_space=pl.ANY)],
        out_shape=[jax.ShapeDtypeStruct((seqs * P_SIZE, width), bf16), jax.ShapeDtypeStruct(state.shape, f32)],
        scratch_shapes=[pltpu.VMEM((heads * TALL, DK), f32)] * 7 + [pltpu.SemaphoreType.DMA],
        cost_estimate=pl.CostEstimate(flops=5_000_000_000, bytes_accessed=state.size * 4, transcendentals=0),
        name="attend",
    )(state, factor, packed, packed, packed, packed, decay, beta, gain.reshape(1, DK))


def pick(index, values):
    chosen = values[-1]
    for at, value in enumerate(values[:-1]):
        chosen = jnp.where(index == at, value, chosen)
    return chosen


def turned_slot(t):
    return pick(t, (0, 2, 1, 3))


ORDER = ((3, 2, 1, 0), (0, 2, 1, 3), (3, 1, 2, 0), (0, 1, 2, 3))


def project_kernel(x_ref, gain_ref, keys, values, thin, wq, wk, wv, wz, wf, ws, state, acc, few_ref, taken, xbuf, w, fs,
                   send, recv, esend, erecv, s_in, s_out, r_scr, u_scr, c_scr, kf, vf,
                   xs, xr, wsem, ps, pr, es, er, ins, outs):
    k, t, g = lax.axis_index("kv"), lax.axis_index("tp"), lax.axis_index("grp")
    depth, width = w.shape[1], w.shape[2]
    rows = x_ref.shape[0]

    def at(kv, tp):
        return {"grp": g, "kv": kv, "tp": tp}

    def remote(src, dst, ss, rs, kv, tp):
        return pltpu.make_async_remote_copy(src, dst, ss, rs, device_id=at(kv, tp), device_id_type=pl.DeviceIdType.MESH)

    loads = [pltpu.make_async_copy(src, w.at[i], wsem.at[i]) for i, src in enumerate((wq, wk, wv, wz))]
    here = pl.ds(k * depth, depth)
    loads += [pltpu.make_async_copy(src.at[:, here], fs.at[i], wsem.at[4 + i]) for i, src in enumerate((wf, ws))]
    slot = turned_slot(t)
    far_t, far_k = turned_slot(k), t
    home = jnp.logical_and(far_k == k, far_t == t)
    first = remote(x_ref, xbuf.at[k], xs.at[0], xr.at[k], far_k, far_t)
    local = pltpu.make_async_copy(x_ref, xbuf.at[k], xr.at[k])

    @pl.when(jnp.logical_not(home))
    def _():
        first.start()

    @pl.when(home)
    def _():
        local.start()

    for load in loads:
        load.start()

    beside = t + 1 - 2 * (t % 2)
    across = (t + 2) % 4

    def arrived(s):
        remote(xbuf.at[s], xbuf.at[s], xs.at[0], xr.at[s], k, beside).wait_recv()

    @pl.when(home)
    def _():
        local.wait()

    @pl.when(jnp.logical_not(home))
    def _():
        arrived(slot)

    over = remote(xbuf.at[slot], xbuf.at[slot], xs.at[1], xr.at[slot], k, across)
    over.start()
    near = remote(xbuf.at[slot], xbuf.at[slot], xs.at[2], xr.at[slot], k, beside)
    near.start()
    def block(r):
        own = r == k
        floated = xbuf[r].astype(f32)
        gained = (floated * gain_ref[k]).astype(bf16)
        squares = floated * floated
        high = squares.astype(bf16)
        rest = (squares - high.astype(f32)).astype(bf16)
        ones = jnp.ones((8, depth), bf16)
        nt = (((1,), (1,)), ((), ()))
        esend[r, 0:16, :] = lax.dot_general(fs[0], gained, nt, preferred_element_type=f32)
        esend[r, 16:32, :] = lax.dot_general(fs[1], gained, nt, preferred_element_type=f32)
        esend[r, 32:40, :] = lax.dot_general(ones, high, nt, preferred_element_type=f32) + lax.dot_general(
            ones, rest, nt, preferred_element_type=f32
        )
        for j in range(4):
            part = jnp.dot(gained, w[j], preferred_element_type=f32)
            cols = slice(j * width, (j + 1) * width)

            @pl.when(own)
            def _():
                acc[:, cols] = part

            @pl.when(jnp.logical_not(own))
            def _():
                send[r, :, cols] = part.astype(bf16)

        relayed = jnp.logical_or(jnp.logical_and(k == 1, r == 3), jnp.logical_and(k == 2, r == 0))

        @pl.when(relayed)
        def _():
            remote(send.at[r], recv.at[4], ps.at[r], pr.at[4], k, beside).wait_recv()

            def add(c, carry):
                at_rows = pl.ds(c * 16, 16)
                send[r, at_rows, :] = (send[r, at_rows, :].astype(f32) + recv[4, at_rows, :].astype(f32)).astype(bf16)
                return carry

            lax.fori_loop(0, rows // 16, add, 0)

        @pl.when(jnp.logical_not(own))
        def _():
            ends = jnp.logical_or(jnp.logical_and(k == 0, r == 3), jnp.logical_and(k == 3, r == 0))
            target = jnp.where(ends, jnp.where(k == 0, 1, 2), r)
            place = jnp.where(ends, 4, k)
            remote(send.at[r], recv.at[place], ps.at[r], pr.at[place], target, t).start()
            remote(esend.at[r], erecv.at[k], es.at[r], er.at[k], r, t).start()

    for load in loads:
        load.wait()
    held_back = jnp.logical_or(jnp.logical_and(k == 1, slot == 3), jnp.logical_and(k == 2, slot == 0))
    early = jnp.logical_and(slot != k, jnp.logical_not(held_back))

    @pl.when(early)
    def _():
        block(slot)

    other = turned_slot(across)
    arrived(other)
    onward = remote(xbuf.at[other], xbuf.at[other], xs.at[3], xr.at[other], k, beside)
    onward.start()
    arrived(turned_slot(beside))
    arrived(turned_slot((beside + 2) % 4))

    def step(i, carry):
        r = pick(k, [pick(i, row) for row in ORDER])

        @pl.when(jnp.logical_not(jnp.logical_and(early, r == slot)))
        def _():
            block(r)

        return carry

    lax.fori_loop(0, 3, step, 0)

    blocks = state.shape[0] // SB
    heads = state.shape[1]

    def fetch(i):
        return pltpu.make_async_copy(state.at[pl.ds(i * SB, SB)], s_in.at[i % 2], ins.at[i % 2])

    def put(i):
        return pltpu.make_async_copy(s_out.at[i % 2], taken.at[pl.ds(i * SB, SB)], outs.at[i % 2])

    def accept(i, carry):
        @pl.when(i + 1 < blocks)
        def _():
            fetch(i + 1).start()

        fetch(i).wait()

        @pl.when(i >= 2)
        def _():
            put(i - 2).wait()

        tall, few_rows = pl.ds(i * TALL, TALL), pl.ds(i * SB, SB)
        accepted_kernel(
            heads, s_in.at[i % 2], keys.at[tall], values.at[tall], thin.at[few_rows], s_out.at[i % 2],
            r_scr, u_scr, c_scr, kf, vf,
        )
        put(i).start()
        return carry

    fetch(0).start()
    lax.fori_loop(0, blocks, accept, 0)
    lax.fori_loop(3, 4, step, 0)
    for i in range(max(blocks - 2, 0), blocks):
        put(i).wait()

    first_wait = jnp.logical_not(home)

    @pl.when(first_wait)
    def _():
        first.wait_send()

    over.wait_send()
    near.wait_send()
    onward.wait_send()

    few_ref[...] = esend[k]
    for src in range(4):

        @pl.when(k != src)
        def _():
            remote(esend.at[src], erecv.at[src], es.at[src], er.at[src], k, beside).wait()
            few_ref[...] += erecv[src]
            remote(send.at[src], recv.at[src], ps.at[src], pr.at[src], k, beside).wait_send()

        @pl.when(jnp.logical_and(k != src, k + src != 3) if src in (0, 3) else k != src)
        def _():
            remote(send.at[src], recv.at[src], ps.at[src], pr.at[src], k, beside).wait_recv()

            def add(c, carry):
                at_rows = pl.ds(c * 16, 16)
                acc[at_rows, :] = acc[at_rows, :] + recv[src, at_rows, :].astype(f32)
                return carry

            lax.fori_loop(0, rows // 16, add, 0)


def project(x, gain, weights, forgetting, strength, state, keys, values, thin):
    rows, depth = x.shape
    width = weights[0].shape[1]
    vmem, hbm = pl.BlockSpec(memory_space=pltpu.VMEM), pl.BlockSpec(memory_space=pl.ANY)
    dma = pltpu.SemaphoreType.DMA
    heads = state.shape[1]
    return pl.pallas_call(
        project_kernel,
        in_specs=[vmem] * 5 + [hbm] * 7,
        out_specs=[vmem, vmem, hbm],
        out_shape=[
            jax.ShapeDtypeStruct((rows, 4 * width), f32),
            jax.ShapeDtypeStruct((40, rows), f32),
            jax.ShapeDtypeStruct(state.shape, f32),
        ],
        scratch_shapes=[
            pltpu.VMEM((4, rows, depth), bf16),
            pltpu.VMEM((4, depth, width), bf16),
            pltpu.VMEM((2, forgetting.shape[1], depth), bf16),
            pltpu.VMEM((4, rows, 4 * width), bf16),
            pltpu.VMEM((5, rows, 4 * width), bf16),
            pltpu.VMEM((4, 40, rows), f32),
            pltpu.VMEM((4, 40, rows), f32),
            pltpu.VMEM((2, SB) + state.shape[1:], f32),
            pltpu.VMEM((2, SB) + state.shape[1:], f32),
            *[pltpu.VMEM((heads * n, DK), f32) for n in (TALL, TALL, SB, TALL, TALL)],
            dma((4,)), dma((4,)), dma((6,)), dma((4,)), dma((5,)), dma((4,)), dma((4,)), dma((2,)), dma((2,)),
        ],
        compiler_params=pltpu.CompilerParams(has_side_effects=True, vmem_limit_bytes=56 * 2**20),
        name="project",
    )(x, gain.reshape(-1, 1, depth), keys, values, thin, *weights, forgetting.T, strength.T, state)


NEAREST = ((0, 1, 2, 3), (1, 0, 2, 3), (2, 3, 1, 0), (3, 2, 1, 0))


def mix_kernel(flat_ref, wo, o_ref, held, w, part, mate, cross, total, wsem, gs, gr, ms, mr, xs, xr, ts, tr):
    k, t, g = lax.axis_index("kv"), lax.axis_index("tp"), lax.axis_index("grp")
    rows = flat_ref.shape[0]

    def remote(src, dst, ss, rs, kv, tp):
        return pltpu.make_async_remote_copy(
            src, dst, ss, rs, device_id={"grp": g, "kv": kv, "tp": tp}, device_id_type=pl.DeviceIdType.MESH
        )

    load = pltpu.make_async_copy(wo, w, wsem.at[0])
    own = pltpu.make_async_copy(flat_ref, held.at[k], wsem.at[1])
    own.start()
    sends = [remote(flat_ref, held.at[k], gs.at[n], gr.at[k], lax.rem(k + n, 4), t) for n in (1, 2, 3)]
    for copy in sends:
        copy.start()
    load.start()
    beside = t + 1 - 2 * (t % 2)
    across = (t + 2) % 4
    diagonal = (beside + 2) % 4
    load.wait()
    own.wait()

    def to_mate(r, n):
        return remote(part.at[r], mate.at[n], ms.at[n], mr.at[n], k, beside)

    def to_cross(r):
        return remote(part.at[r], cross, xs, xr, k, across)

    def step(i, carry):
        r = pick(k, [pick(i, row) for row in NEAREST])

        @pl.when(r != k)
        def _():
            remote(held.at[r], held.at[r], gs.at[0], gr.at[r], r, t).wait_recv()

        part[r] = jnp.dot(held[r], w[...], preferred_element_type=f32).astype(bf16)
        sink = turned_slot(r)

        @pl.when(sink == beside)
        def _():
            to_mate(r, 0).start()

        @pl.when(sink == diagonal)
        def _():
            to_mate(r, 1).start()

        @pl.when(sink == across)
        def _():
            to_mate(r, 1).wait_recv()

            def add(c, carry):
                at_rows = pl.ds(c * 16, 16)
                part[r, at_rows, :] = (part[r, at_rows, :].astype(f32) + mate[1, at_rows, :].astype(f32)).astype(bf16)
                return carry

            lax.fori_loop(0, rows // 16, add, 0)
            to_cross(r).start()

        return carry

    lax.fori_loop(0, 4, step, 0)
    mine = turned_slot(t)
    to_mate(mine, 0).wait_recv()
    to_cross(mine).wait_recv()

    def add(c, carry):
        at_rows = pl.ds(c * 16, 16)
        total[at_rows, :] = (
            part[mine, at_rows, :].astype(f32) + mate[0, at_rows, :].astype(f32) + cross[at_rows, :].astype(f32)
        ).astype(bf16)
        return carry

    lax.fori_loop(0, rows // 16, add, 0)
    home = jnp.logical_and(mine == k, t == k)
    last = remote(total, o_ref, ts, tr, mine, k)
    local = pltpu.make_async_copy(total, o_ref, tr)

    @pl.when(home)
    def _():
        local.start()
        local.wait()

    @pl.when(jnp.logical_not(home))
    def _():
        last.start()
        last.wait()

    for copy in sends:
        copy.wait_send()
    to_mate(0, 0).wait_send()
    to_mate(0, 1).wait_send()
    to_cross(0).wait_send()


def mix(flat, final):
    rows, width = flat.shape
    cols = final.shape[1]
    vmem, hbm = pl.BlockSpec(memory_space=pltpu.VMEM), pl.BlockSpec(memory_space=pl.ANY)
    dma = pltpu.SemaphoreType.DMA
    return pl.pallas_call(
        mix_kernel,
        in_specs=[vmem, hbm],
        out_specs=vmem,
        out_shape=jax.ShapeDtypeStruct((rows, cols), bf16),
        scratch_shapes=[
            pltpu.VMEM((4, rows, width), bf16),
            pltpu.VMEM((width, cols), bf16),
            pltpu.VMEM((4, rows, cols), bf16),
            pltpu.VMEM((2, rows, cols), bf16),
            pltpu.VMEM((rows, cols), bf16),
            pltpu.VMEM((rows, cols), bf16),
            dma((2,)), dma((4,)), dma((4,)), dma((2,)), dma((2,)), dma, dma, dma, dma,
        ],
        compiler_params=pltpu.CompilerParams(has_side_effects=True, vmem_limit_bytes=56 * 2**20),
        name="mix",
    )(flat, final)


def on_device(
    n_kv,
    n_tp,
    candidate_embeddings,
    incoming_rms_scaling,
    probe_projector,
    address_projector,
    content_projector,
    sigmoid_mask_matrix,
    forgetting_projector,
    strength_projector_matrix,
    channel_forgetting_rates,
    forgetting_offset,
    extra_forgetting,
    outgoing_rms_scaling,
    final_projector,
    memory_matrix,
    earlier_addresses,
    earlier_contents,
    earlier_strengths,
    earlier_forgetting,
    admitted_counts,
):
    rows, local_cols = candidate_embeddings.shape
    features = incoming_rms_scaling.shape[0]
    depth, width = probe_projector.shape
    heads = width // DK
    seqs = rows // P_SIZE
    k_index, t_index = lax.axis_index("kv"), lax.axis_index("tp")

    def thin(values):
        return values.reshape(seqs, P_SIZE * heads)

    weights = (probe_projector, address_projector, content_projector, sigmoid_mask_matrix)
    earlier = (
        memory_matrix,
        earlier_addresses.reshape(rows, width),
        earlier_contents.reshape(rows, width),
        jnp.concatenate(
            [thin(earlier_forgetting), thin(earlier_strengths), admitted_counts.astype(f32).reshape(seqs, 1)], axis=1
        ),
    )
    if n_kv == 4 and n_tp == 4:
        summed, few, taken = project(
            candidate_embeddings, incoming_rms_scaling, weights, forgetting_projector, strength_projector_matrix, *earlier
        )
        columns = forgetting_projector.shape[1]
        few = [lax.dynamic_slice_in_dim(few, n * columns + t_index * heads, heads) for n in range(2)] + [few[2 * columns : 2 * columns + 1]]
        few = jnp.concatenate(few, axis=0).T
    else:
        every = lax.all_gather(candidate_embeddings, "tp", axis=1, tiled=True)
        every = lax.all_to_all(every, "kv", split_axis=1, concat_axis=0, tiled=True)
        gain_part = lax.dynamic_slice_in_dim(incoming_rms_scaling, k_index * depth, depth)
        floated = every.astype(f32)
        gained = (floated * gain_part).astype(bf16)
        decay_cols = lax.dynamic_slice(forgetting_projector, (k_index * depth, t_index * heads), (depth, heads))
        beta_cols = lax.dynamic_slice(strength_projector_matrix, (k_index * depth, t_index * heads), (depth, heads))
        few = jnp.concatenate(
            [
                jnp.dot(gained, jnp.concatenate([decay_cols, beta_cols], axis=1), preferred_element_type=f32),
                jnp.sum(floated * floated, axis=1, keepdims=True),
            ],
            axis=1,
        )
        few = lax.psum_scatter(few, "kv", scatter_dimension=0, tiled=True)
        partial = jnp.concatenate(
            [jnp.dot(gained, w, preferred_element_type=f32).astype(bf16) for w in weights], axis=1
        )
        summed = lax.psum_scatter(partial, "kv", scatter_dimension=0, tiled=True).astype(f32)
        taken = accepted(*earlier)
    factor = lax.rsqrt(few[:, 2 * heads :] / features + epsilon)
    few = few[:, : 2 * heads] * factor
    decay_in = few[:, :heads].reshape(seqs, P_SIZE, heads)
    beta = jax.nn.sigmoid(few[:, heads:].reshape(seqs, P_SIZE, heads))
    decay = -jnp.exp(channel_forgetting_rates) * jax.nn.softplus(decay_in + forgetting_offset) + extra_forgetting
    flat, taken = attend(taken, summed, factor, thin(decay), thin(beta), outgoing_rms_scaling)
    if n_kv == 4 and n_tp == 4:
        mixed = mix(flat, final_projector)
    else:
        gathered = lax.all_gather(flat, "kv", axis=0, tiled=True)
        terms = jnp.dot(gathered, final_projector, preferred_element_type=f32).astype(bf16)
        terms = lax.all_to_all(terms, "kv", split_axis=0, concat_axis=1, tiled=True)
        mixed = lax.psum_scatter(terms, "tp", scatter_dimension=1, tiled=True)
    return (mixed, taken)


def solution(mesh):
    row, per_head = P(("grp", "kv"), "tp"), P(("grp", "kv"), None, "tp")
    four = P(("grp", "kv"), None, "tp", None)
    weight = P("kv", "tp")
    state = P(("grp", "kv"), "tp", None, None)
    in_specs = (
        row, P(), weight, weight, weight, weight, P(), P(), P("tp"), P("tp"), per_head, P(),
        P("tp", "kv"), state, four, four, per_head, per_head, P(("grp", "kv")),
    )
    body = functools.partial(on_device, mesh.shape["kv"], mesh.shape["tp"])
    return jax.shard_map(body, mesh=mesh, in_specs=in_specs, out_specs=(row, state), check_vma=False)
```
